512 devices in a mesh: dp: 4 (over x), kv: 64 (over z, y), tp: 2 (over core).
Axes of the slice: x: 4, y: 4, z: 16, core: 2. Of those that a mesh axis runs over, the one named last changes fastest.
Arguments:
- tokens: bfloat16 [512, 4096], P('dp', 'kv'), parts along dimension 0, may hold values from -16 to 16
- gain_mix: float32 [4096], P('kv'), may hold values from 0.1 to 1.9
- w_query: bfloat16 [4096, 2048], P('kv', 'tp'), may hold values from -0.09375 to 0.09375
- w_key: bfloat16 [4096, 2048], P('kv', 'tp'), may hold values from -0.09375 to 0.09375
- w_value: bfloat16 [4096, 2048], P('kv', 'tp'), may hold values from -0.09375 to 0.09375
- w_igate: bfloat16 [4096, 16], P('kv', 'tp'), may hold values from -0.09375 to 0.09375
- w_fgate: bfloat16 [4096, 16], P('kv', 'tp'), may hold values from -0.09375 to 0.09375
- bias_igate: float32 [16], P('tp'), may hold values from -1 to 1
- bias_fgate: float32 [16], P('tp'), may hold values from -1 to 4
- memory: float32 [512, 16, 128, 128], P(('dp', 'kv'), 'tp'), parts along dimension 0, may hold values from -0.8 to 0.8
- normalizer: float32 [512, 16, 128], P(('dp', 'kv'), 'tp'), parts along dimension 0, may hold values from -0.8 to 0.8
- stabilizer: float32 [512, 16], P(('dp', 'kv'), 'tp'), parts along dimension 0, may hold values from -1.5 to 1.5
- w_output: bfloat16 [2048, 4096], P('tp', 'kv'), may hold values from -0.125 to 0.125
- gain_mlp: float32 [4096], replicated, may hold values from 0.1 to 1.9
- w_gate: bfloat16 [4096, 11264], P(None, ('kv', 'tp')), may hold values from -0.09375 to 0.09375
- w_up: bfloat16 [4096, 11264], P(None, ('kv', 'tp')), may hold values from -0.09375 to 0.09375
- w_down: bfloat16 [11264, 4096], P(('kv', 'tp')), may hold values from -0.21875 to 0.21875
Outputs:
- mixed: bfloat16 [512, 4096], P('dp', ('kv', 'tp')), parts along dimension 0
- memory_next: float32 [512, 16, 128, 128], P(('dp', 'kv'), 'tp'), parts along dimension 0
- normalizer_next: float32 [512, 16, 128], P(('dp', 'kv'), 'tp'), parts along dimension 0
- stabilizer_next: float32 [512, 16], P(('dp', 'kv'), 'tp'), parts along dimension 0
The draws below stay inside these ranges and needn't reach their ends.
There are 4 independent parts, one for each index of `dp`. The reference program is written for one: setup_inputs(seed, part) draws one part's arguments, and reference() takes and returns one part's arrays. A program takes and returns all parts, laid end to end along the dimension named above; an argument that names none is the same for every part. Nothing has to cross between parts.
All inputs are finite; a program needn't handle non-finite values.
Results may differ from the reference program's by a relative error of at most 0.014.
Values may be sent and summed in bfloat16 or wider, within the bound.
No kernel may reach another device: no remote copies, remote signals or barrier semaphores. Data moves between devices by JAX's collectives and lax.ppermute only.
A program may use at most 64 MiB of HBM per device.

```python
import math
import jax
import jax.numpy as jnp
from jax import lax

D = 4096
HEADS = 16
HEAD_DIM = 128
FF = 11264
BATCH = 128
N_TP = 2


def draw_tokens(key, part):
    key_base, key_rows, key_rough = jax.random.split(key, 3)
    ramp = jnp.exp(jnp.linspace(math.log(0.5), math.log(2.0), D)).reshape(1, D)
    rough = jax.random.uniform(key_rough, (1, D), jnp.float32, 0.5, 1.5)
    row_scale = jnp.exp(jax.random.uniform(key_rows, (BATCH, 1), jnp.float32, math.log(0.3), math.log(3.0)))
    base = jax.random.normal(key_base, (BATCH, D), jnp.float32)
    return jnp.clip(base * row_scale * ramp * rough, -16.0, 16.0).astype(jnp.bfloat16)


def strengthened(array, stream_key, source, target, blocks, factor):
    owner, partner = [(jnp.arange(array.shape[dim]) // (array.shape[dim] // blocks)).reshape([-1 if axis == dim else 1 for axis in range(array.ndim)]) for dim in (source, target)]
    chosen = jax.random.permutation(stream_key, blocks)[partner]
    strong = (owner == chosen) | (owner == (partner + blocks // 2) % blocks)
    return jnp.where(strong, factor * array, array)


def block_levels(stream_key, extent, cuts, least, largest):
    loudness, own = 1.0, jax.random.fold_in(stream_key, 6)
    for position, blocks in cuts:
        steps = jnp.exp(jax.random.uniform(jax.random.fold_in(own, position), (blocks,), jnp.float32, least / len(cuts), largest / len(cuts)))
        loudness = loudness * jnp.repeat(steps, extent[position] // blocks).reshape([-1 if axis == position else 1 for axis in range(len(extent))])
    return loudness


def scatter_about(rng, shape, spread, limit, cuts=(), held_as=jnp.bfloat16):
    array = jax.random.normal(rng, shape, jnp.float32) * spread
    if len(cuts) > 0:
        array = block_levels(rng, shape, cuts, -0.22, 0.18) * array
    return jnp.clip(array, min=-limit, max=limit).astype(held_as)


def gaussian_with(own_key, shape, width, reach, cuts, heavy, dtype=jnp.bfloat16):
    drawn = width * jax.random.normal(own_key, shape, jnp.float32)
    if cuts:
        drawn = drawn * block_levels(own_key, shape, cuts, -0.22, 0.18)
    return jnp.clip(strengthened(drawn, jax.random.fold_in(own_key, 3), *heavy), -reach, reach).astype(dtype)


def setup_inputs(seed: int = 0, part: int = 0) -> dict:
    arg_keys = jax.random.split(jax.random.key(seed), 18)
    part_splits = jax.random.split(jax.random.fold_in(arg_keys[17], part), 18)
    return {
        "tokens": draw_tokens(jax.random.fold_in(jax.random.fold_in(arg_keys[17], part), 71), part),
        "gain_mix": jnp.clip(1.0 + 0.18 * jax.random.normal(arg_keys[1], (D,), jnp.float32), 0.1, 1.9),
        "w_query": scatter_about(arg_keys[2], (D, HEADS * HEAD_DIM), D ** -0.5, 0.09375, ((0, 64), (1, 2))),
        "w_key": scatter_about(arg_keys[3], (D, HEADS * HEAD_DIM), D ** -0.5, 0.09375, ((0, 64), (1, 2))),
        "w_value": scatter_about(arg_keys[4], (D, HEADS * HEAD_DIM), D ** -0.5, 0.09375, ((0, 64), (1, 2))),
        "w_igate": scatter_about(arg_keys[5], (D, HEADS), D ** -0.5, 0.09375, ((0, 64), (1, 2))),
        "w_fgate": scatter_about(arg_keys[6], (D, HEADS), D ** -0.5, 0.09375, ((0, 64), (1, 2))),
        "bias_igate": jnp.clip(jax.random.uniform(arg_keys[7], (HEADS,), jnp.float32, -1.0, 1.0) * block_levels(arg_keys[7], (HEADS,), ((0, 2),), -0.4, 0.0), -1.0, 1.0),
        "bias_fgate": jnp.clip(-1.0 + 5.0 * jax.random.uniform(arg_keys[8], (HEADS,), jnp.float32) ** block_levels(arg_keys[8], (HEADS,), ((0, 2),), -0.2, 0.2), -1.0, 4.0),
        "memory": scatter_about(part_splits[9], (BATCH, HEADS, HEAD_DIM, HEAD_DIM), 0.1, 0.8, ((0, 64), (1, 2)), jnp.float32),
        "normalizer": scatter_about(part_splits[10], (BATCH, HEADS, HEAD_DIM), 0.1, 0.8, ((0, 64), (1, 2)), jnp.float32),
        "stabilizer": jnp.clip(jax.random.uniform(part_splits[11], (BATCH, HEADS), jnp.float32, -1.5, 1.5) * block_levels(part_splits[11], (BATCH, HEADS), ((0, 64), (1, 2)), -0.4, 0.0), -1.5, 1.5),
        "w_output": scatter_about(arg_keys[12], (HEADS * HEAD_DIM, D), (HEADS * HEAD_DIM) ** -0.5, 0.125, ((0, 2), (1, 64))),
        "gain_mlp": jnp.clip(1.0 + 0.18 * jax.random.normal(arg_keys[13], (D,), jnp.float32), 0.1, 1.9),
        "w_gate": scatter_about(arg_keys[14], (D, FF), D ** -0.5, 0.09375, ((1, 128),)),
        "w_up": scatter_about(arg_keys[15], (D, FF), D ** -0.5, 0.09375, ((1, 128),)),
        "w_down": gaussian_with(arg_keys[16], (FF, D), FF ** -0.5, 0.21875, ((0, 128),), (0, 1, 128, 5.5)),
    }


epsilon = 1e-06

def cell_update(queries, key_proj, values, in_gate, log_forget, memory, normalizer, stabilizer, head_count):
    batch_rows = queries.shape[0]
    query_heads = queries.astype(jnp.float32).reshape(batch_rows, head_count, -1)
    head_dim = query_heads.shape[2]
    key_heads = key_proj.astype(jnp.float32).reshape(batch_rows, head_count, head_dim) * head_dim ** (-0.5)
    value_heads = values.astype(jnp.float32).reshape(batch_rows, head_count, head_dim)
    stab_next = jnp.maximum(stabilizer + log_forget, in_gate)
    keeping = jnp.exp(stabilizer + log_forget - stab_next)
    fresh_weight = jnp.exp(in_gate - stab_next)
    memory_next = keeping[:, :, None, None] * memory + fresh_weight[:, :, None, None] * value_heads[:, :, :, None] * key_heads[:, :, None, :]
    norm_next = keeping[:, :, None] * normalizer + fresh_weight[:, :, None] * key_heads
    numerator = jnp.einsum('bhvk,bhk->bhv', memory_next, query_heads, precision=lax.Precision.HIGHEST)
    denominator = jnp.einsum('bhk,bhk->bh', norm_next, query_heads, precision=lax.Precision.HIGHEST)
    denominator = jnp.maximum(jnp.abs(denominator), jnp.exp(-stab_next))
    hidden = (numerator / denominator[:, :, None]).reshape(batch_rows, -1).astype(jnp.bfloat16)
    return (hidden, memory_next, norm_next, stab_next)

def reference(tokens, gain_mix, w_query, w_key, w_value, w_igate, w_fgate, bias_igate, bias_fgate, memory, normalizer, stabilizer, w_output, gain_mlp, w_gate, w_up, w_down):
    tok_float = tokens.astype(jnp.float32)
    scaling = lax.rsqrt(lax.optimization_barrier(jnp.mean(tok_float * tok_float, axis=1, keepdims=True)) + epsilon)
    scaled = (tok_float * gain_mix).astype(jnp.bfloat16)

    def project(weight):
        return scaling * jnp.dot(scaled, weight, preferred_element_type=jnp.float32)
    queries = project(w_query).astype(jnp.bfloat16)
    key_proj = project(w_key).astype(jnp.bfloat16)
    values = project(w_value).astype(jnp.bfloat16)
    in_gate = project(w_igate) + bias_igate
    log_forget = jax.nn.log_sigmoid(project(w_fgate) + bias_fgate)
    hidden, memory_next, norm_next, stab_next = cell_update(queries, key_proj, values, in_gate, log_forget, memory, normalizer, stabilizer, HEADS)
    block_cols = w_output.shape[0] // N_TP
    branch = jnp.zeros(tokens.shape, jnp.float32)
    for block_index in range(N_TP):
        lower = block_index * block_cols
        partial_out = jnp.dot(hidden[:, lower:lower + block_cols], w_output[lower:lower + block_cols], preferred_element_type=jnp.float32)
        rounded = lax.optimization_barrier(partial_out.astype(jnp.bfloat16))
        branch = branch + rounded.astype(jnp.float32)
    residual = (tok_float + branch).astype(jnp.bfloat16)
    res_float = residual.astype(jnp.float32)
    scaling_mlp = lax.rsqrt(lax.optimization_barrier(jnp.mean(res_float * res_float, axis=1, keepdims=True)) + epsilon)
    normed = (res_float * scaling_mlp * gain_mlp).astype(jnp.bfloat16)
    gate_act = jnp.dot(normed, w_gate, preferred_element_type=jnp.float32)
    up_act = jnp.dot(normed, w_up, preferred_element_type=jnp.float32)
    activated = (jax.nn.silu(gate_act) * up_act).astype(jnp.bfloat16)
    mixed = (res_float + jnp.dot(activated, w_down, preferred_element_type=jnp.float32)).astype(jnp.bfloat16)
    return (mixed, memory_next, norm_next, stab_next)
```

```python
import jax
import jax.numpy as jnp
from jax import lax
from jax.experimental import pallas as pl
from jax.experimental.pallas import tpu as pltpu
from jax.sharding import Mesh
from jax.sharding import PartitionSpec as P

D = 4096
KV = ("kv_0", "kv_1")
DP_KV = ("dp", "kv_0", "kv_1")
KV_TP = ("kv_0", "kv_1", "tp")
Z, Y = 16, 4
ROWS = 128
HALF = 32
BLOCK = Z * HALF
PADDED = BLOCK + 16
epsilon = 1e-06
f32 = jnp.float32
bf16 = jnp.bfloat16


def exchanged(x, axis):
    return lax.all_to_all(x, axis, split_axis=0, concat_axis=0, tiled=True)


def swapped(x):
    return lax.ppermute(x, "tp", [(0, 1), (1, 0)])


def contracted(a, b, dim_a, dim_b):
    return lax.dot_general(a, b, (((dim_a,), (dim_b,)), ((), ())), preferred_element_type=f32)


def natural_row(i):
    return 8 * ((i // 2) % Z) + 2 * (i // 32) + i % 2


def row_selection(transposed):
    a = lax.broadcasted_iota(jnp.int32, (ROWS, ROWS), 0)
    b = lax.broadcasted_iota(jnp.int32, (ROWS, ROWS), 1)
    if transposed:
        hit = natural_row(a) == b
    else:
        hit = a == natural_row(b)
    return jnp.where(hit, 1.0, 0.0).astype(bf16)


def high_low(x):
    lane = lax.broadcasted_iota(jnp.int32, x.shape, 1)
    high = x.astype(bf16)
    low = (x - high.astype(f32)).astype(bf16)
    return jnp.where(lane < 64, high.astype(f32), low.astype(f32)).astype(bf16)


def project_kernel(tok_ref, gain_ref, wq_ref, wk_ref, wv_ref, wi_ref, wf_ref, out_ref, tok_out_ref):
    perm = row_selection(False)
    tok = jnp.dot(tok_ref[...], perm, preferred_element_type=f32)
    tok_out_ref[...] = tok.astype(bf16)
    scaled = (tok * gain_ref[...]).astype(bf16)
    for n, ref in enumerate((wq_ref, wk_ref, wv_ref)):
        part = contracted(scaled, ref[...], 0, 0).astype(bf16)
        out_ref[:, :, 1024 * n : 1024 * (n + 1)] = part.reshape(Y, 32, 1024)
    gates = jnp.concatenate([wi_ref[...].astype(f32), wf_ref[...].astype(f32)], axis=0)
    rest = jnp.zeros((48, 64), f32)
    gates = jnp.concatenate([gates, rest, gates, rest], axis=0).astype(bf16)
    extra = contracted(scaled, gates, 0, 1)
    squares = tok * tok
    high = squares.astype(bf16)
    low = (squares - high.astype(f32)).astype(bf16)
    lane = lax.broadcasted_iota(jnp.int32, (64, 128), 1)
    ones = jnp.where(lane % 64 == 16, 1.0, 0.0).astype(bf16)
    extra = extra + contracted(high, ones, 0, 0) + contracted(low, ones, 0, 0)
    out_ref[:, :, 3072:] = high_low(extra).reshape(Y, 32, 128)


def sum_y_kernel(in_ref, out_ref):
    for n in range(3):
        cut = slice(1024 * n, 1024 * (n + 1))
        total = in_ref[0, :, cut].astype(f32)
        for y in range(1, Y):
            total = total + in_ref[y, :, cut].astype(f32)
        out_ref[:, :, cut] = total.astype(bf16).reshape(Z, 2, 1024)
    total = in_ref[0, :, 3072:].astype(f32)
    for y in range(1, Y):
        total = total + in_ref[y, :, 3072:].astype(f32)
    total = total + jnp.concatenate([total[:, 64:], total[:, :64]], axis=1)
    out_ref[:, :, 3072:] = high_low(total).reshape(Z, 2, 128)


def cell_update(queries, key_proj, values, in_gate, log_forget, memory, normalizer, stabilizer):
    batch_rows, head_count = stabilizer.shape
    query_heads = queries.astype(f32).reshape(batch_rows, head_count, -1)
    head_dim = query_heads.shape[2]
    key_heads = key_proj.astype(f32).reshape(batch_rows, head_count, head_dim) * head_dim ** (-0.5)
    value_heads = values.astype(f32).reshape(batch_rows, head_count, head_dim)
    stab_next = jnp.maximum(stabilizer + log_forget, in_gate)
    keeping = jnp.exp(stabilizer + log_forget - stab_next)
    fresh_weight = jnp.exp(in_gate - stab_next)
    memory_next = (
        keeping[:, :, None, None] * memory
        + fresh_weight[:, :, None, None] * value_heads[:, :, :, None] * key_heads[:, :, None, :]
    )
    norm_next = keeping[:, :, None] * normalizer + fresh_weight[:, :, None] * key_heads
    numerator = jnp.einsum(
        "bhvk,bhk->bhv", memory_next, query_heads, precision=lax.Precision.HIGHEST
    )
    denominator = jnp.einsum("bhk,bhk->bh", norm_next, query_heads, precision=lax.Precision.HIGHEST)
    denominator = jnp.maximum(jnp.abs(denominator), jnp.exp(-stab_next))
    hidden = (numerator / denominator[:, :, None]).astype(bf16)
    return (hidden, memory_next, norm_next, stab_next)


def gain_kernel(in_ref, gain_ref, out_ref):
    squares = jnp.zeros((HALF, ROWS), f32)
    for z in range(Z):
        x = in_ref[z].astype(f32)
        squares = squares + x * x
        scaled = (x * gain_ref[z]).astype(bf16)
        for y in range(Y):
            out_ref[y, HALF * z : HALF * (z + 1), :] = scaled
    total = jnp.sum(squares, axis=0, keepdims=True)
    high = total.astype(bf16).astype(f32)
    low = (total - high).astype(bf16).astype(f32)
    row = lax.broadcasted_iota(jnp.int32, (16, ROWS), 0)
    tail = jnp.where(row == 0, high, jnp.where(row == 1, low, 0.0)).astype(bf16)
    for y in range(Y):
        out_ref[y, BLOCK:, :] = tail


def mlp_kernel(core_ref, own_ref, other_ref, wg_ref, wu_ref, wd_ref, keep_ref, send_ref, x_ref):
    first = core_ref[0] == 0
    squares = jnp.zeros((16, ROWS), f32)
    for y in range(Y):
        squares = squares + own_ref[y, BLOCK:, :].astype(f32) + other_ref[y, BLOCK:, :].astype(f32)
    scaling = lax.rsqrt(jnp.sum(squares, axis=0, keepdims=True) / D + epsilon)

    for y in range(Y):
        for z in range(Z):
            at = 64 * (Y * z + y)
            own = own_ref[y, HALF * z : HALF * (z + 1), :]
            other = other_ref[y, HALF * z : HALF * (z + 1), :]
            x_ref[at : at + HALF, :] = jnp.where(first, own, other)
            x_ref[at + HALF : at + 64, :] = jnp.where(first, other, own)
    x = x_ref[...]
    gate = scaling * jnp.dot(wg_ref[...], x, preferred_element_type=f32)
    up = scaling * jnp.dot(wu_ref[...], x, preferred_element_type=f32)
    activated = (gate * jax.nn.sigmoid(gate) * up).astype(bf16)
    for m in range(2 * Z):
        part = contracted(wd_ref[:, 128 * m : 128 * (m + 1)], activated, 0, 0)
        z = m // 2
        for pair in range(2):
            y = 2 * (m % 2) + pair
            lower = part[64 * pair : 64 * pair + HALF]
            upper = part[64 * pair + HALF : 64 * pair + 64]
            keep_ref[y, HALF * z : HALF * (z + 1), :] = jnp.where(first, lower, upper)
            send_ref[y, HALF * z : HALF * (z + 1), :] = jnp.where(first, upper, lower).astype(bf16)


def finish_kernel(in_ref, res_ref, out_ref):
    total = res_ref[...].astype(f32)
    acc = in_ref[0].astype(f32)
    for z in range(1, Z):
        acc = acc + in_ref[z].astype(f32)
    mixed = (total + acc).astype(bf16)
    out_ref[...] = jnp.dot(mixed, row_selection(True), preferred_element_type=f32).astype(bf16)


def called(kernel, out_shape, flops=0, bytes_accessed=0, **kw):
    return pl.pallas_call(
        kernel,
        out_shape=out_shape,
        cost_estimate=pl.CostEstimate(
            flops=flops, bytes_accessed=bytes_accessed, transcendentals=0
        ),
        **kw,
    )


def local(
    tokens,
    gain_mix,
    w_query,
    w_key,
    w_value,
    w_igate,
    w_fgate,
    bias_igate,
    bias_fgate,
    memory,
    normalizer,
    stabilizer,
    w_output,
    gain_mlp,
    w_gate,
    w_up,
    w_down,
):
    core = lax.axis_index("tp")
    shape = jax.ShapeDtypeStruct
    gain_rows = jnp.broadcast_to(gain_mix[:, None], (64, ROWS))
    partials, tok = called(
        project_kernel,
        (shape((Y, 32, 3200), bf16), shape((64, ROWS), bf16)),
        flops=2 * 64 * 128 * 3200,
    )(tokens.T, gain_rows, w_query, w_key, w_value, w_igate.T, w_fgate.T)
    partials = exchanged(partials, "kv_1")
    partials = called(sum_y_kernel, shape((Z, 2, 3200), bf16), flops=10**6)(partials)
    partials = exchanged(partials, "kv_0")
    sums = partials.astype(f32).sum(axis=0)
    extra = sums[:, 3072:3136] + sums[:, 3136:]
    scaling = lax.rsqrt(extra[:, 16:17] / D + epsilon)
    queries = (scaling * sums[:, :1024]).astype(bf16)
    key_proj = (scaling * sums[:, 1024:2048]).astype(bf16)
    values = (scaling * sums[:, 2048:3072]).astype(bf16)
    in_gate = scaling * extra[:, :8] + bias_igate
    log_forget = jax.nn.log_sigmoid(scaling * extra[:, 8:16] + bias_fgate)
    hidden, memory_next, norm_next, stab_next = cell_update(
        queries, key_proj, values, in_gate, log_forget, memory, normalizer, stabilizer
    )
    hidden = jnp.broadcast_to(hidden.reshape(1, 16, 128), (Z, 16, 128))
    hidden = exchanged(hidden, "kv_0").reshape(32, 1024)
    hidden = exchanged(jnp.broadcast_to(hidden[None], (Y, 32, 1024)), "kv_1")
    hidden = hidden.reshape(ROWS, 1024)
    part = contracted(w_output.T, hidden, 1, 1).astype(bf16)
    arrived = swapped(lax.dynamic_slice_in_dim(part, HALF * (1 - core), HALF, 0))
    kept = lax.dynamic_slice_in_dim(part, HALF * core, HALF, 0)
    branch = kept.astype(f32) + arrived.astype(f32)
    tok_half = lax.dynamic_slice_in_dim(tok, HALF * core, HALF, 0)
    residual = (tok_half.astype(f32) + branch).astype(bf16)

    spread = exchanged(jnp.broadcast_to(residual[None], (Z, HALF, ROWS)), "kv_0")
    gain = lax.dynamic_slice(
        gain_mlp.reshape(Z, Y, 2, HALF), (0, lax.axis_index("kv_1"), core, 0), (Z, 1, 1, HALF)
    )
    gain = jnp.broadcast_to(gain.reshape(Z, HALF, 1), (Z, HALF, ROWS))
    spread = called(gain_kernel, shape((Y, PADDED, ROWS), bf16), flops=10**6)(spread, gain)
    spread = exchanged(spread, "kv_1")
    other = swapped(spread)
    keep, send = called(
        mlp_kernel,
        (shape((Y, BLOCK, ROWS), f32), shape((Y, BLOCK, ROWS), bf16)),
        flops=6 * 128 * 88 * 4096,
        in_specs=[pl.BlockSpec(memory_space=pltpu.SMEM)]
        + [pl.BlockSpec(memory_space=pltpu.VMEM)] * 5,
        scratch_shapes=[pltpu.VMEM((D, ROWS), bf16)],
    )(core.astype(jnp.int32).reshape(1), spread, other, w_gate.T, w_up.T, w_down)
    terms = (keep + swapped(send).astype(f32)).astype(bf16)
    terms = exchanged(terms, "kv_1").astype(f32).sum(axis=0).astype(bf16)
    terms = exchanged(terms.reshape(Z, HALF, ROWS), "kv_0")
    mixed = called(finish_kernel, shape((HALF, ROWS), bf16), flops=10**6)(terms, residual)
    return (mixed.T, memory_next, norm_next, stab_next)


def solution(mesh):
    torus = Mesh(
        mesh.devices.reshape(mesh.shape["dp"], Z, Y, mesh.shape["tp"]),
        ("dp", "kv_0", "kv_1", "tp"),
    )
    in_specs = (
        P("dp", KV),
        P(KV),
        P(KV, "tp"),
        P(KV, "tp"),
        P(KV, "tp"),
        P(KV, "tp"),
        P(KV, "tp"),
        P("tp"),
        P("tp"),
        P(DP_KV, "tp", None, None),
        P(DP_KV, "tp", None),
        P(DP_KV, "tp"),
        P("tp", KV),
        P(),
        P(None, KV_TP),
        P(None, KV_TP),
        P(KV_TP, None),
    )
    out_specs = (P("dp", KV_TP), P(DP_KV, "tp", None, None), P(DP_KV, "tp", None), P(DP_KV, "tp"))
    return jax.shard_map(local, mesh=torus, in_specs=in_specs, out_specs=out_specs, check_vma=False)
```

```python
import jax
import jax.numpy as jnp
from jax import lax
from jax.experimental import pallas as pl
from jax.experimental.pallas import tpu as pltpu
from jax.sharding import Mesh
from jax.sharding import PartitionSpec as P

D = 4096
KV = ("kv_0", "kv_1")
DP_KV = ("dp", "kv_0", "kv_1")
KV_TP = ("kv_0", "kv_1", "tp")
Z, Y = 16, 4
ROWS = 128
HALF = 32
BLOCK = Z * HALF
PADDED = BLOCK + 16
epsilon = 1e-06
f32 = jnp.float32
bf16 = jnp.bfloat16


def exchanged(x, axis):
    return lax.all_to_all(x, axis, split_axis=0, concat_axis=0, tiled=True)


def swapped(x):
    return lax.ppermute(x, "tp", [(0, 1), (1, 0)])


def contracted(a, b, dim_a, dim_b):
    return lax.dot_general(a, b, (((dim_a,), (dim_b,)), ((), ())), preferred_element_type=f32)


def natural_row(i):
    return 8 * ((i // 2) % Z) + 2 * (i // 32) + i % 2


def row_selection(transposed):
    a = lax.broadcasted_iota(jnp.int32, (ROWS, ROWS), 0)
    b = lax.broadcasted_iota(jnp.int32, (ROWS, ROWS), 1)
    if transposed:
        hit = natural_row(a) == b
    else:
        hit = a == natural_row(b)
    return jnp.where(hit, 1.0, 0.0).astype(bf16)


def high_low(x):
    lane = lax.broadcasted_iota(jnp.int32, x.shape, 1)
    high = x.astype(bf16)
    low = (x - high.astype(f32)).astype(bf16)
    return jnp.where(lane < 64, high.astype(f32), low.astype(f32)).astype(bf16)


def column_of(row, count, offset=0):
    lane = lax.broadcasted_iota(jnp.int32, (count, row.shape[1]), 1)
    at = lax.broadcasted_iota(jnp.int32, (count, row.shape[1]), 0)
    return jnp.sum(jnp.where(lane == at + offset, row, 0.0), axis=1, keepdims=True)


def project_kernel(
    tok_ref, gain_ref, wi_ref, wf_ref, wq_ref, wk_ref, wv_ref, out_ref, tok_out_ref, w_ref, sems
):
    copies = [
        pltpu.make_async_copy(ref, w_ref.at[n], sems.at[n])
        for n, ref in enumerate((wq_ref, wk_ref, wv_ref))
    ]
    for copy in copies:
        copy.start()
    tok = jnp.dot(tok_ref[...], row_selection(False), preferred_element_type=f32)
    tok_out_ref[...] = tok.astype(bf16)
    scaled = (tok * column_of(gain_ref[...], 64)).astype(bf16)
    gates = jnp.concatenate([wi_ref[...].astype(f32), wf_ref[...].astype(f32)], axis=0)
    rest = jnp.zeros((48, 64), f32)
    gates = jnp.concatenate([gates, rest, gates, rest], axis=0).astype(bf16)
    extra = contracted(scaled, gates, 0, 1)
    squares = tok * tok
    high = squares.astype(bf16)
    low = (squares - high.astype(f32)).astype(bf16)
    lane = lax.broadcasted_iota(jnp.int32, (64, 128), 1)
    ones = jnp.where(lane % 64 == 16, 1.0, 0.0).astype(bf16)
    extra = extra + contracted(high, ones, 0, 0) + contracted(low, ones, 0, 0)
    out_ref[:, :, 3072:] = high_low(extra).reshape(Y, 32, 128)
    for n in range(3):
        copies[n].wait()
        part = contracted(scaled, w_ref[n], 0, 0).astype(bf16)
        out_ref[:, :, 1024 * n : 1024 * (n + 1)] = part.reshape(Y, 32, 1024)


def sum_y_kernel(in_ref, out_ref):
    for n in range(3):
        cut = slice(1024 * n, 1024 * (n + 1))
        total = in_ref[0, :, cut].astype(f32)
        for y in range(1, Y):
            total = total + in_ref[y, :, cut].astype(f32)
        out_ref[:, :, cut] = total.astype(bf16).reshape(Z, 2, 1024)
    total = in_ref[0, :, 3072:].astype(f32)
    for y in range(1, Y):
        total = total + in_ref[y, :, 3072:].astype(f32)
    total = total + jnp.concatenate([total[:, 64:], total[:, :64]], axis=1)
    out_ref[:, :, 3072:] = high_low(total).reshape(Z, 2, 128)


def by_head(x):
    count = x.shape[1]
    return jnp.concatenate(
        [jnp.broadcast_to(x[0:1], (8, count)), jnp.broadcast_to(x[1:2], (8, count))], axis=0
    )


def picked(x, offset):
    lane = lax.broadcasted_iota(jnp.int32, x.shape, 1)
    head = lax.broadcasted_iota(jnp.int32, x.shape, 0) % 8
    return jnp.sum(jnp.where(lane == head + offset, x, 0.0), axis=1, keepdims=True)


def cell_kernel(
    in_ref, bi_ref, bf_ref, mem_ref, norm_ref, stab_ref,
    hid_ref, mem_out_ref, norm_out_ref, stab_out_ref, rows_ref,
):
    sums = in_ref[0].astype(f32)
    for z in range(1, Z):
        sums = sums + in_ref[z].astype(f32)
    for n in range(3):
        for j in range(2):
            for h in range(8):
                at = 1024 * n + 128 * h
                rows_ref[n, 8 * j + h : 8 * j + h + 1, :] = sums[j : j + 1, at : at + 128]
    extra = by_head(sums[:, 3072:3136] + sums[:, 3136:3200])
    lane = lax.broadcasted_iota(jnp.int32, extra.shape, 1)
    total = jnp.sum(jnp.where(lane == 16, extra, 0.0), axis=1, keepdims=True)
    scaling = lax.rsqrt(total / D + epsilon)
    in_gate = scaling * picked(extra, 0) + picked(jnp.broadcast_to(bi_ref[...], (16, 8)), 0)
    forget = scaling * picked(extra, 8) + picked(jnp.broadcast_to(bf_ref[...], (16, 8)), 0)
    log_forget = jnp.minimum(forget, 0.0) - jnp.log1p(jnp.exp(-jnp.abs(forget)))
    kept = picked(by_head(stab_ref[...]), 0) + log_forget
    stab_next = jnp.maximum(kept, in_gate)
    keeping = jnp.exp(kept - stab_next)
    fresh = jnp.exp(in_gate - stab_next)
    queries = (scaling * rows_ref[0]).astype(bf16).astype(f32)
    keys = (scaling * rows_ref[1]).astype(bf16).astype(f32) * 128 ** (-0.5)
    values = (scaling * rows_ref[2]).astype(bf16).astype(f32)
    norm_next = keeping * norm_ref[...] + fresh * keys
    norm_out_ref[...] = norm_next
    denominator = jnp.sum(norm_next * queries, axis=1, keepdims=True)
    denominator = jnp.maximum(jnp.abs(denominator), jnp.exp(-stab_next))
    own = lax.broadcasted_iota(jnp.int32, (16, 8), 1)
    head = lax.broadcasted_iota(jnp.int32, (16, 8), 0) % 8
    spread = jnp.where(own == head, stab_next, 0.0)
    stab_out_ref[0:1, :] = jnp.sum(spread[:8], axis=0, keepdims=True)
    stab_out_ref[1:2, :] = jnp.sum(spread[8:], axis=0, keepdims=True)
    added = jnp.concatenate([fresh * values, jnp.zeros((112, 128), f32)], axis=0).T
    column = lax.broadcasted_iota(jnp.int32, (128, 128), 1)
    numerator = jnp.zeros((128, 128), f32)
    for i in range(16):
        update = added[:, i : i + 1] * keys[i : i + 1, :]
        mem_next = keeping[i : i + 1, :] * mem_ref[i] + update
        mem_out_ref[i] = mem_next
        read = jnp.sum(mem_next * queries[i : i + 1, :], axis=1, keepdims=True)
        numerator = jnp.where(column == i, read, numerator)
    hidden = (numerator.T[:16] / denominator).astype(bf16)
    for z in range(Z):
        hid_ref[z] = hidden


def spread_kernel(in_ref, out_ref):
    for n in range(out_ref.shape[0]):
        out_ref[n] = in_ref[...]


def residual_kernel(core_ref, part_ref, arrived_ref, tok_ref, out_ref, spread_ref):
    first = core_ref[0] == 0
    part = jnp.where(first, part_ref[:HALF], part_ref[HALF:]).astype(f32)
    tok = jnp.where(first, tok_ref[:HALF], tok_ref[HALF:]).astype(f32)
    residual = (tok + (part + arrived_ref[...].astype(f32))).astype(bf16)
    out_ref[...] = residual
    for z in range(Z):
        spread_ref[z] = residual


def gain_kernel(core_ref, in_ref, gain_ref, out_ref):
    squares = jnp.zeros((HALF, ROWS), f32)
    for z in range(Z):
        x = in_ref[z].astype(f32)
        squares = squares + x * x
        gain = column_of(gain_ref[z : z + 1, :], HALF, core_ref[1])
        scaled = (x * gain).astype(bf16)
        for y in range(Y):
            out_ref[y, HALF * z : HALF * (z + 1), :] = scaled
    total = jnp.sum(squares, axis=0, keepdims=True)
    high = total.astype(bf16).astype(f32)
    low = (total - high).astype(bf16).astype(f32)
    row = lax.broadcasted_iota(jnp.int32, (16, ROWS), 0)
    tail = jnp.where(row == 0, high, jnp.where(row == 1, low, 0.0)).astype(bf16)
    for y in range(Y):
        out_ref[y, BLOCK:, :] = tail


def mlp_kernel(core_ref, own_ref, other_ref, wg_ref, wu_ref, wd_ref, keep_ref, send_ref, x_ref):
    first = core_ref[0] == 0
    squares = jnp.zeros((16, ROWS), f32)
    for y in range(Y):
        squares = squares + own_ref[y, BLOCK:, :].astype(f32) + other_ref[y, BLOCK:, :].astype(f32)
    scaling = lax.rsqrt(jnp.sum(squares, axis=0, keepdims=True) / D + epsilon)

    for y in range(Y):
        for z in range(Z):
            at = 64 * (Y * z + y)
            own = own_ref[y, HALF * z : HALF * (z + 1), :]
            other = other_ref[y, HALF * z : HALF * (z + 1), :]
            x_ref[at : at + HALF, :] = jnp.where(first, own, other)
            x_ref[at + HALF : at + 64, :] = jnp.where(first, other, own)
    x = x_ref[...]
    gate = scaling * jnp.dot(wg_ref[...], x, preferred_element_type=f32)
    up = scaling * jnp.dot(wu_ref[...], x, preferred_element_type=f32)
    activated = (gate * jax.nn.sigmoid(gate) * up).astype(bf16)
    for m in range(2 * Z):
        part = contracted(wd_ref[:, 128 * m : 128 * (m + 1)], activated, 0, 0)
        z = m // 2
        for pair in range(2):
            y = 2 * (m % 2) + pair
            lower = part[64 * pair : 64 * pair + HALF]
            upper = part[64 * pair + HALF : 64 * pair + 64]
            keep_ref[y, HALF * z : HALF * (z + 1), :] = jnp.where(first, lower, upper)
            send_ref[y, HALF * z : HALF * (z + 1), :] = jnp.where(first, upper, lower).astype(bf16)


def finish_kernel(in_ref, res_ref, out_ref):
    total = res_ref[...].astype(f32)
    acc = in_ref[0].astype(f32)
    for z in range(1, Z):
        acc = acc + in_ref[z].astype(f32)
    mixed = (total + acc).astype(bf16)
    out_ref[...] = jnp.dot(mixed, row_selection(True), preferred_element_type=f32).astype(bf16)


def called(kernel, out_shape, flops=0, grant=16, **kw):
    return pl.pallas_call(
        kernel,
        out_shape=out_shape,
        cost_estimate=pl.CostEstimate(flops=flops, bytes_accessed=10**6, transcendentals=0),
        compiler_params=pltpu.CompilerParams(vmem_limit_bytes=grant * 2**20),
        **kw,
    )


IN_VMEM = pl.BlockSpec(memory_space=pltpu.VMEM)
IN_SMEM = pl.BlockSpec(memory_space=pltpu.SMEM)
IN_HBM = pl.BlockSpec(memory_space=pltpu.HBM)


def local(
    tokens,
    gain_mix,
    w_query,
    w_key,
    w_value,
    w_igate,
    w_fgate,
    bias_igate,
    bias_fgate,
    memory,
    normalizer,
    stabilizer,
    w_output,
    gain_mlp,
    w_gate,
    w_up,
    w_down,
):
    core = lax.axis_index("tp")
    place = jnp.stack([core, 64 * lax.axis_index("kv_1") + HALF * core]).astype(jnp.int32)
    shape = jax.ShapeDtypeStruct
    partials, tok = called(
        project_kernel,
        (shape((Y, 32, 3200), bf16), shape((64, ROWS), bf16)),
        flops=2 * 64 * 128 * 3200,
        in_specs=[IN_VMEM] * 4 + [IN_HBM] * 3,
        scratch_shapes=[pltpu.VMEM((3, 64, 1024), bf16), pltpu.SemaphoreType.DMA((3,))],
    )(tokens.T, gain_mix.reshape(1, 64), w_igate.T, w_fgate.T, w_query, w_key, w_value)
    partials = exchanged(partials, "kv_1")
    partials = called(sum_y_kernel, shape((Z, 2, 3200), bf16), flops=10**6)(partials)
    partials = exchanged(partials, "kv_0")
    hidden, memory_next, norm_next, stab_next = called(
        cell_kernel,
        (
            shape((Z, 16, 128), bf16),
            shape((16, 128, 128), f32),
            shape((16, 128), f32),
            shape((2, 8), f32),
        ),
        flops=10**7,
        scratch_shapes=[pltpu.VMEM((3, 16, 128), f32)],
    )(
        partials,
        bias_igate.reshape(1, 8),
        bias_fgate.reshape(1, 8),
        memory.reshape(16, 128, 128),
        normalizer.reshape(16, 128),
        stabilizer,
    )
    hidden = exchanged(hidden, "kv_0").reshape(32, 1024)
    hidden = called(spread_kernel, shape((Y, 32, 1024), bf16), flops=10**6)(hidden)
    hidden = exchanged(hidden, "kv_1").reshape(ROWS, 1024)
    part = contracted(w_output.T, hidden, 1, 1).astype(bf16)
    arrived = swapped(lax.dynamic_slice_in_dim(part, HALF * (1 - core), HALF, 0))
    residual, spread = called(
        residual_kernel,
        (shape((HALF, ROWS), bf16), shape((Z, HALF, ROWS), bf16)),
        flops=10**6,
        in_specs=[IN_SMEM] + [IN_VMEM] * 3,
    )(place, part, arrived, tok)
    spread = exchanged(spread, "kv_0")
    spread = called(
        gain_kernel,
        shape((Y, PADDED, ROWS), bf16),
        flops=10**6,
        in_specs=[IN_SMEM] + [IN_VMEM] * 2,
    )(place, spread, gain_mlp.reshape(Z, 256))
    spread = exchanged(spread, "kv_1")
    other = swapped(spread)
    keep, send = called(
        mlp_kernel,
        (shape((Y, BLOCK, ROWS), f32), shape((Y, BLOCK, ROWS), bf16)),
        flops=6 * 128 * 88 * 4096,
        in_specs=[IN_SMEM] + [IN_VMEM] * 5,
        scratch_shapes=[pltpu.VMEM((D, ROWS), bf16)],
    )(place, spread, other, w_gate.T, w_up.T, w_down)
    terms = (keep + swapped(send).astype(f32)).astype(bf16)
    terms = exchanged(terms, "kv_1").astype(f32).sum(axis=0).astype(bf16)
    terms = exchanged(terms.reshape(Z, HALF, ROWS), "kv_0")
    mixed = called(finish_kernel, shape((HALF, ROWS), bf16), flops=10**6)(terms, residual)
    return (
        mixed.T,
        memory_next.reshape(2, 8, 128, 128),
        norm_next.reshape(2, 8, 128),
        stab_next,
    )


def solution(mesh):
    torus = Mesh(
        mesh.devices.reshape(mesh.shape["dp"], Z, Y, mesh.shape["tp"]),
        ("dp", "kv_0", "kv_1", "tp"),
    )
    in_specs = (
        P("dp", KV),
        P(KV),
        P(KV, "tp"),
        P(KV, "tp"),
        P(KV, "tp"),
        P(KV, "tp"),
        P(KV, "tp"),
        P("tp"),
        P("tp"),
        P(DP_KV, "tp", None, None),
        P(DP_KV, "tp", None),
        P(DP_KV, "tp"),
        P("tp", KV),
        P(),
        P(None, KV_TP),
        P(None, KV_TP),
        P(KV_TP, None),
    )
    out_specs = (P("dp", KV_TP), P(DP_KV, "tp", None, None), P(DP_KV, "tp", None), P(DP_KV, "tp"))
    return jax.shard_map(local, mesh=torus, in_specs=in_specs, out_specs=out_specs, check_vma=False)
```

```python
import jax
import jax.numpy as jnp
from jax import lax
from jax.experimental import pallas as pl
from jax.experimental.pallas import tpu as pltpu
from jax.sharding import Mesh
from jax.sharding import PartitionSpec as P

D = 4096
KV = ("kv_0", "kv_1")
DP_KV = ("dp", "kv_0", "kv_1")
KV_TP = ("kv_0", "kv_1", "tp")
Z, Y = 16, 4
ROWS = 128
HALF = 32
BLOCK = Z * HALF
epsilon = 1e-06
f32 = jnp.float32
bf16 = jnp.bfloat16


def exchanged(x, axis):
    return lax.all_to_all(x, axis, split_axis=0, concat_axis=0, tiled=True)


def swapped(x):
    return lax.ppermute(x, "tp", [(0, 1), (1, 0)])


def contracted(a, b, dim_a, dim_b):
    return lax.dot_general(a, b, (((dim_a,), (dim_b,)), ((), ())), preferred_element_type=f32)


def natural_row(i):
    return 8 * ((i // 2) % Z) + 2 * (i // 32) + i % 2


def final_row(i):
    return 8 * (i % Z) + 2 * ((i // Z) % Y) + i // 64


def row_selection(transposed, natural_row=natural_row):
    a = lax.broadcasted_iota(jnp.int32, (ROWS, ROWS), 0)
    b = lax.broadcasted_iota(jnp.int32, (ROWS, ROWS), 1)
    if transposed:
        hit = natural_row(a) == b
    else:
        hit = a == natural_row(b)
    return jnp.where(hit, 1.0, 0.0).astype(bf16)


def high_low(x):
    lane = lax.broadcasted_iota(jnp.int32, x.shape, 1)
    high = x.astype(bf16)
    low = (x - high.astype(f32)).astype(bf16)
    return jnp.where(lane < 64, high.astype(f32), low.astype(f32)).astype(bf16)


def column_of(row, count, offset=0):
    lane = lax.broadcasted_iota(jnp.int32, (count, row.shape[1]), 1)
    at = lax.broadcasted_iota(jnp.int32, (count, row.shape[1]), 0)
    return jnp.sum(jnp.where(lane == at + offset, row, 0.0), axis=1, keepdims=True)


def project_kernel(
    tok_ref, gain_ref, wi_ref, wf_ref, wq_ref, wk_ref, wv_ref, out_ref, w_ref, sems
):
    copies = [
        pltpu.make_async_copy(ref, w_ref.at[n], sems.at[n])
        for n, ref in enumerate((wq_ref, wk_ref, wv_ref))
    ]
    for copy in copies:
        copy.start()
    tok = jnp.dot(tok_ref[...], row_selection(False), preferred_element_type=f32)
    rows = contracted(row_selection(True), tok_ref[...], 1, 1).astype(bf16)
    out_ref[:, :, 3200:] = jnp.concatenate([rows, rows], axis=1).reshape(Y, 32, 128)
    scaled = (tok * column_of(gain_ref[...], 64)).astype(bf16)
    gates = jnp.concatenate([wi_ref[...].astype(f32), wf_ref[...].astype(f32)], axis=0)
    rest = jnp.zeros((48, 64), f32)
    gates = jnp.concatenate([gates, rest, gates, rest], axis=0).astype(bf16)
    extra = contracted(scaled, gates, 0, 1)
    squares = tok * tok
    high = squares.astype(bf16)
    low = (squares - high.astype(f32)).astype(bf16)
    lane = lax.broadcasted_iota(jnp.int32, (64, 128), 1)
    ones = jnp.where(lane % 64 == 16, 1.0, 0.0).astype(bf16)
    extra = extra + contracted(high, ones, 0, 0) + contracted(low, ones, 0, 0)
    out_ref[:, :, 3072:3200] = high_low(extra).reshape(Y, 32, 128)
    for n in range(3):
        copies[n].wait()
        part = contracted(scaled, w_ref[n], 0, 0).astype(bf16)
        out_ref[:, :, 1024 * n : 1024 * (n + 1)] = part.reshape(Y, 32, 1024)


def sum_y_kernel(in_ref, out_ref, tok_ref):
    for y in range(Y):
        tok_ref[:, 64 * y : 64 * (y + 1)] = in_ref[y, :, 3200:3264]
    for n in range(3):
        cut = slice(1024 * n, 1024 * (n + 1))
        total = in_ref[0, :, cut].astype(f32)
        for y in range(1, Y):
            total = total + in_ref[y, :, cut].astype(f32)
        out_ref[:, :, cut] = total.astype(bf16).reshape(Z, 2, 1024)
    total = in_ref[0, :, 3072:3200].astype(f32)
    for y in range(1, Y):
        total = total + in_ref[y, :, 3072:3200].astype(f32)
    total = total + jnp.concatenate([total[:, 64:], total[:, :64]], axis=1)
    out_ref[:, :, 3072:] = high_low(total).reshape(Z, 2, 128)


def by_head(x):
    count = x.shape[1]
    return jnp.concatenate(
        [jnp.broadcast_to(x[0:1], (8, count)), jnp.broadcast_to(x[1:2], (8, count))], axis=0
    )


def picked(x, offset):
    lane = lax.broadcasted_iota(jnp.int32, x.shape, 1)
    head = lax.broadcasted_iota(jnp.int32, x.shape, 0) % 8
    return jnp.sum(jnp.where(lane == head + offset, x, 0.0), axis=1, keepdims=True)


def cell_kernel(
    in_ref, bi_ref, bf_ref, mem_ref, norm_ref, stab_ref,
    hid_ref, mem_out_ref, norm_out_ref, stab_out_ref, rows_ref,
):
    sums = in_ref[0].astype(f32)
    for z in range(1, Z):
        sums = sums + in_ref[z].astype(f32)
    for n in range(3):
        for j in range(2):
            for h in range(8):
                at = 1024 * n + 128 * h
                rows_ref[n, 8 * j + h : 8 * j + h + 1, :] = sums[j : j + 1, at : at + 128]
    extra = by_head(sums[:, 3072:3136] + sums[:, 3136:3200])
    lane = lax.broadcasted_iota(jnp.int32, extra.shape, 1)
    total = jnp.sum(jnp.where(lane == 16, extra, 0.0), axis=1, keepdims=True)
    scaling = lax.rsqrt(total / D + epsilon)
    in_gate = scaling * picked(extra, 0) + picked(jnp.broadcast_to(bi_ref[...], (16, 8)), 0)
    forget = scaling * picked(extra, 8) + picked(jnp.broadcast_to(bf_ref[...], (16, 8)), 0)
    log_forget = jnp.minimum(forget, 0.0) - jnp.log1p(jnp.exp(-jnp.abs(forget)))
    kept = picked(by_head(stab_ref[...]), 0) + log_forget
    stab_next = jnp.maximum(kept, in_gate)
    keeping = jnp.exp(kept - stab_next)
    fresh = jnp.exp(in_gate - stab_next)
    queries = (scaling * rows_ref[0]).astype(bf16).astype(f32)
    keys = (scaling * rows_ref[1]).astype(bf16).astype(f32) * 128 ** (-0.5)
    values = (scaling * rows_ref[2]).astype(bf16).astype(f32)
    norm_next = keeping * norm_ref[...] + fresh * keys
    norm_out_ref[...] = norm_next
    denominator = jnp.sum(norm_next * queries, axis=1, keepdims=True)
    denominator = jnp.maximum(jnp.abs(denominator), jnp.exp(-stab_next))
    own = lax.broadcasted_iota(jnp.int32, (16, 8), 1)
    head = lax.broadcasted_iota(jnp.int32, (16, 8), 0) % 8
    spread = jnp.where(own == head, stab_next, 0.0)
    stab_out_ref[0:1, :] = jnp.sum(spread[:8], axis=0, keepdims=True)
    stab_out_ref[1:2, :] = jnp.sum(spread[8:], axis=0, keepdims=True)
    added = jnp.concatenate([fresh * values, jnp.zeros((112, 128), f32)], axis=0).T
    column = lax.broadcasted_iota(jnp.int32, (128, 128), 1)
    numerator = jnp.zeros((128, 128), f32)
    for i in range(16):
        update = added[:, i : i + 1] * keys[i : i + 1, :]
        mem_next = keeping[i : i + 1, :] * mem_ref[i] + update
        mem_out_ref[i] = mem_next
        read = jnp.sum(mem_next * queries[i : i + 1, :], axis=1, keepdims=True)
        numerator = jnp.where(column == i, read, numerator)
    hidden = (numerator.T[:16] / denominator).astype(bf16)
    for z in range(Z):
        hid_ref[2 * z] = hidden[:8]
        hid_ref[2 * z + 1] = hidden[8:]


def spread_kernel(in_ref, out_ref):
    for n in range(out_ref.shape[0]):
        out_ref[n] = in_ref[...]


def residual_kernel(
    place_ref, hid_ref, tok_ref, w0_ref, w1_ref, w2_ref, w3_ref, other_ref, spread_ref, parts_ref
):
    first = place_ref[0] == 0
    lower, upper = hid_ref[:, :1024], hid_ref[:, 1024:]
    own = jnp.where(first, lower, upper)
    other = jnp.where(first, upper, lower)
    for step, ref in enumerate((w0_ref, w1_ref, w2_ref, w3_ref)):
        part = contracted(own, ref[...], 1, 1).astype(bf16).astype(f32)
        part = part + contracted(other, other_ref[step], 1, 1).astype(bf16).astype(f32)
        parts_ref[(place_ref[2] + Y - step) % Y] = part
    branch = jnp.concatenate([parts_ref[y] for y in range(Y)], axis=1)
    at = lax.broadcasted_iota(jnp.int32, (Z, 32), 0)
    row = lax.broadcasted_iota(jnp.int32, (Z, 32), 1)
    chosen = jnp.where(row == 2 * at + place_ref[0], 1.0, 0.0).astype(bf16)
    tok = jnp.dot(chosen, tok_ref[...], preferred_element_type=f32)
    residual = (tok + branch).astype(bf16)
    for z in range(Z):
        spread_ref[z] = residual


def mlp_kernel(
    place_ref, own_ref, other_ref, gain_ref, wg_ref, wu_ref, wd_ref,
    keep_ref, send_ref, res_ref, x_ref, block_ref,
):
    first = place_ref[0] == 0
    squares = [jnp.zeros((Z, 256), f32) for _ in range(2 * Y)]
    for z in range(Z):
        gain = gain_ref[z : z + 1, :]
        for y in range(Y):
            own = own_ref[y, Z * z : Z * (z + 1), :].astype(f32)
            other = other_ref[y, Z * z : Z * (z + 1), :].astype(f32)
            for n, x in enumerate((jnp.where(first, own, other), jnp.where(first, other, own))):
                at = Y * n + y
                squares[at] = squares[at] + x * x
                x_ref[Z * at : Z * (at + 1), 256 * z : 256 * (z + 1)] = (x * gain).astype(bf16)
    total = jnp.sum(jnp.concatenate(squares, axis=0), axis=1, keepdims=True)
    scaling = lax.rsqrt(total / D + epsilon)
    scaling = jnp.broadcast_to(scaling, (ROWS, ROWS)).T[0:1]

    here = pl.multiple_of(Z * place_ref[3], Z)
    for y in range(Y):
        own = own_ref[y, pl.ds(here, Z), :]
        other = other_ref[y, pl.ds(here, Z), :]
        block_ref[Z * y : Z * (y + 1), :] = jnp.where(first, own, other)
        block_ref[64 + Z * y : 64 + Z * (y + 1), :] = jnp.where(first, other, own)
    at = lax.broadcasted_iota(jnp.int32, (HALF, 256), 0)
    lane = lax.broadcasted_iota(jnp.int32, (HALF, 256), 1)
    chosen = jnp.where(lane == at + place_ref[1], 1.0, 0.0).astype(bf16)
    res_ref[...] = contracted(chosen, block_ref[...], 1, 1).astype(bf16)

    x = x_ref[...]
    gate = scaling * contracted(wg_ref[...], x, 1, 1)
    up = scaling * contracted(wu_ref[...], x, 1, 1)
    activated = (gate * jax.nn.sigmoid(gate) * up).astype(bf16)
    for m in range(2 * Z):
        part = contracted(wd_ref[:, 128 * m : 128 * (m + 1)], activated, 0, 0)
        z = m // 2
        for pair in range(2):
            y = 2 * (m % 2) + pair
            lower = part[64 * pair : 64 * pair + HALF]
            upper = part[64 * pair + HALF : 64 * pair + 64]
            keep_ref[y, HALF * z : HALF * (z + 1), :] = jnp.where(first, lower, upper)
            send_ref[y, HALF * z : HALF * (z + 1), :] = jnp.where(first, upper, lower).astype(bf16)


def finish_kernel(in_ref, res_ref, out_ref):
    total = res_ref[...].astype(f32)
    acc = in_ref[0].astype(f32)
    for z in range(1, Z):
        acc = acc + in_ref[z].astype(f32)
    mixed = (total + acc).astype(bf16)
    out_ref[...] = jnp.dot(mixed, row_selection(True, final_row), preferred_element_type=f32).astype(bf16)


def called(kernel, out_shape, flops=0, grant=16, **kw):
    return pl.pallas_call(
        kernel,
        out_shape=out_shape,
        cost_estimate=pl.CostEstimate(flops=flops, bytes_accessed=10**6, transcendentals=0),
        compiler_params=pltpu.CompilerParams(vmem_limit_bytes=grant * 2**20),
        **kw,
    )


IN_VMEM = pl.BlockSpec(memory_space=pltpu.VMEM)
IN_SMEM = pl.BlockSpec(memory_space=pltpu.SMEM)
IN_HBM = pl.BlockSpec(memory_space=pltpu.HBM)


def local(
    tokens,
    gain_mix,
    w_query,
    w_key,
    w_value,
    w_igate,
    w_fgate,
    bias_igate,
    bias_fgate,
    memory,
    normalizer,
    stabilizer,
    w_output,
    gain_mlp,
    w_gate,
    w_up,
    w_down,
):
    core = lax.axis_index("tp")
    at_z, at_y = lax.axis_index("kv_0"), lax.axis_index("kv_1")
    place = jnp.stack([core, 64 * at_y + HALF * core, at_y, at_z]).astype(jnp.int32)
    shape = jax.ShapeDtypeStruct
    partials = called(
        project_kernel,
        shape((Y, 32, 3328), bf16),
        flops=2 * 64 * 128 * 3200,
        grant=60,
        in_specs=[IN_VMEM] * 4 + [IN_HBM] * 3,
        scratch_shapes=[pltpu.VMEM((3, 64, 1024), bf16), pltpu.SemaphoreType.DMA((3,))],
    )(tokens.T, gain_mix.reshape(1, 64), w_igate.T, w_fgate.T, w_query, w_key, w_value)
    partials = exchanged(partials, "kv_1")
    partials, tok = called(
        sum_y_kernel, (shape((Z, 2, 3200), bf16), shape((32, 256), bf16)), flops=10**6
    )(partials)
    w_own, partials = lax.optimization_barrier((w_output.T, partials))
    with jax.named_scope("sums"):
        partials = exchanged(partials, "kv_0")
    w_all = [w_own]
    for step in range(1, Y):
        with jax.named_scope("columns" + str(step)):
            w_all.append(lax.ppermute(w_own, "kv_1", [(i, (i + step) % Y) for i in range(Y)]))
    with jax.named_scope("pair"):
        w_other = swapped(jnp.stack(w_all))
    hidden, memory_next, norm_next, stab_next = called(
        cell_kernel,
        (
            shape((2 * Z, 8, 128), bf16),
            shape((16, 128, 128), f32),
            shape((16, 128), f32),
            shape((2, 8), f32),
        ),
        flops=10**7,
        scratch_shapes=[pltpu.VMEM((3, 16, 128), f32)],
    )(
        partials,
        bias_igate.reshape(1, 8),
        bias_fgate.reshape(1, 8),
        memory.reshape(16, 128, 128),
        normalizer.reshape(16, 128),
        stabilizer,
    )
    with jax.named_scope("heads"):
        hidden = exchanged(hidden, ("kv_0", "tp"))
    spread = called(
        residual_kernel,
        shape((Z, Z, 256), bf16),
        flops=10**7,
        in_specs=[IN_SMEM] + [IN_VMEM] * 7,
        scratch_shapes=[pltpu.VMEM((Y, Z, 64), f32)],
    )(place, hidden.reshape(Z, 2048), tok, *w_all, w_other)
    with jax.named_scope("gather"):
        spread = exchanged(spread, "kv_0").reshape(256, 256)
    spread = called(spread_kernel, shape((Y, 256, 256), bf16), flops=10**6)(spread)
    spread = exchanged(spread, "kv_1")
    other = swapped(spread)
    keep, send, residual = called(
        mlp_kernel,
        (
            shape((Y, BLOCK, ROWS), f32),
            shape((Y, BLOCK, ROWS), bf16),
            shape((HALF, ROWS), bf16),
        ),
        flops=6 * 128 * 88 * 4096,
        in_specs=[IN_SMEM] + [IN_VMEM] * 6,
        scratch_shapes=[pltpu.VMEM((ROWS, D), bf16), pltpu.VMEM((ROWS, 256), bf16)],
    )(place, spread, other, gain_mlp.reshape(Z, 256), w_gate.T, w_up.T, w_down)
    terms = (keep + swapped(send).astype(f32)).astype(bf16)
    terms = exchanged(terms, "kv_1").astype(f32).sum(axis=0).astype(bf16)
    terms = exchanged(terms.reshape(Z, HALF, ROWS), "kv_0")
    mixed = called(finish_kernel, shape((HALF, ROWS), bf16), flops=10**6)(terms, residual)
    return (
        mixed.T,
        memory_next.reshape(2, 8, 128, 128),
        norm_next.reshape(2, 8, 128),
        stab_next,
    )


def solution(mesh):
    torus = Mesh(
        mesh.devices.reshape(mesh.shape["dp"], Z, Y, mesh.shape["tp"]),
        ("dp", "kv_0", "kv_1", "tp"),
    )
    in_specs = (
        P("dp", KV),
        P(KV),
        P(KV, "tp"),
        P(KV, "tp"),
        P(KV, "tp"),
        P(KV, "tp"),
        P(KV, "tp"),
        P("tp"),
        P("tp"),
        P(DP_KV, "tp", None, None),
        P(DP_KV, "tp", None),
        P(DP_KV, "tp"),
        P("tp", KV),
        P(),
        P(None, KV_TP),
        P(None, KV_TP),
        P(KV_TP, None),
    )
    out_specs = (P("dp", KV_TP), P(DP_KV, "tp", None, None), P(DP_KV, "tp", None), P(DP_KV, "tp"))
    return jax.shard_map(local, mesh=torus, in_specs=in_specs, out_specs=out_specs, check_vma=False)
```

```python
import jax
import jax.numpy as jnp
from jax import lax
from jax.experimental import pallas as pl
from jax.experimental.pallas import tpu as pltpu
from jax.sharding import Mesh
from jax.sharding import PartitionSpec as P


D = 4096
KV = ("kv_0", "kv_1")
DP_KV = ("dp", "kv_0", "kv_1")
KV_TP = ("kv_0", "kv_1", "tp")
Z, Y = 16, 4
ROWS = 128
HALF = 32
BLOCK = Z * HALF
epsilon = 1e-06
f32 = jnp.float32
bf16 = jnp.bfloat16


def exchanged(x, axis):
    return lax.all_to_all(x, axis, split_axis=0, concat_axis=0, tiled=True)


def swapped(x):
    return lax.ppermute(x, "tp", [(0, 1), (1, 0)])


def contracted(a, b, dim_a, dim_b):
    return lax.dot_general(a, b, (((dim_a,), (dim_b,)), ((), ())), preferred_element_type=f32)


def natural_row(i):
    return 8 * ((i // 2) % Z) + 2 * (i // 32) + i % 2


def final_row(i):
    return 8 * (i % Z) + 2 * ((i // Z) % Y) + i // 64


def row_selection(transposed, natural_row=natural_row):
    a = lax.broadcasted_iota(jnp.int32, (ROWS, ROWS), 0)
    b = lax.broadcasted_iota(jnp.int32, (ROWS, ROWS), 1)
    if transposed:
        hit = natural_row(a) == b
    else:
        hit = a == natural_row(b)
    return jnp.where(hit, 1.0, 0.0).astype(bf16)


def high_low(x):
    lane = lax.broadcasted_iota(jnp.int32, x.shape, 1)
    high = x.astype(bf16)
    low = (x - high.astype(f32)).astype(bf16)
    return jnp.where(lane < 64, high.astype(f32), low.astype(f32)).astype(bf16)


def column_of(row, count, offset=0):
    lane = lax.broadcasted_iota(jnp.int32, (count, row.shape[1]), 1)
    at = lax.broadcasted_iota(jnp.int32, (count, row.shape[1]), 0)
    return jnp.sum(jnp.where(lane == at + offset, row, 0.0), axis=1, keepdims=True)


def project_kernel(
    tok_ref, gain_ref, wi_ref, wf_ref, wq_ref, wk_ref, wv_ref, out_ref, w_ref, sems
):
    copies = [
        pltpu.make_async_copy(ref, w_ref.at[n], sems.at[n])
        for n, ref in enumerate((wq_ref, wk_ref, wv_ref))
    ]
    for copy in copies:
        copy.start()
    tok = jnp.dot(tok_ref[...], row_selection(False), preferred_element_type=f32)
    rows = contracted(row_selection(True), tok_ref[...], 1, 1).astype(bf16)
    out_ref[:, :, 3200:] = jnp.concatenate([rows, rows], axis=1).reshape(Y, 32, 128)
    scaled = (tok * column_of(gain_ref[...], 64)).astype(bf16)
    gates = jnp.concatenate([wi_ref[...].astype(f32), wf_ref[...].astype(f32)], axis=0)
    rest = jnp.zeros((48, 64), f32)
    gates = jnp.concatenate([gates, rest, gates, rest], axis=0).astype(bf16)
    extra = contracted(scaled, gates, 0, 1)
    squares = tok * tok
    high = squares.astype(bf16)
    low = (squares - high.astype(f32)).astype(bf16)
    lane = lax.broadcasted_iota(jnp.int32, (64, 128), 1)
    ones = jnp.where(lane % 64 == 16, 1.0, 0.0).astype(bf16)
    extra = extra + contracted(high, ones, 0, 0) + contracted(low, ones, 0, 0)
    out_ref[:, :, 3072:3200] = high_low(extra).reshape(Y, 32, 128)
    for n in range(3):
        copies[n].wait()
        part = contracted(scaled, w_ref[n], 0, 0).astype(bf16)
        out_ref[:, :, 1024 * n : 1024 * (n + 1)] = part.reshape(Y, 32, 1024)


def sum_y_kernel(in_ref, out_ref, tok_ref):
    for y in range(Y):
        tok_ref[:, 64 * y : 64 * (y + 1)] = in_ref[y, :, 3200:3264]
    for n in range(3):
        cut = slice(1024 * n, 1024 * (n + 1))
        total = in_ref[0, :, cut].astype(f32)
        for y in range(1, Y):
            total = total + in_ref[y, :, cut].astype(f32)
        out_ref[:, :, cut] = total.astype(bf16).reshape(Z, 2, 1024)
    total = in_ref[0, :, 3072:3200].astype(f32)
    for y in range(1, Y):
        total = total + in_ref[y, :, 3072:3200].astype(f32)
    total = total + jnp.concatenate([total[:, 64:], total[:, :64]], axis=1)
    out_ref[:, :, 3072:] = high_low(total).reshape(Z, 2, 128)


def by_head(x):
    count = x.shape[1]
    return jnp.concatenate(
        [jnp.broadcast_to(x[0:1], (8, count)), jnp.broadcast_to(x[1:2], (8, count))], axis=0
    )


def picked(x, offset):
    lane = lax.broadcasted_iota(jnp.int32, x.shape, 1)
    head = lax.broadcasted_iota(jnp.int32, x.shape, 0) % 8
    return jnp.sum(jnp.where(lane == head + offset, x, 0.0), axis=1, keepdims=True)


def cell_kernel(
    in_ref, bi_ref, bf_ref, mem_ref, norm_ref, stab_ref,
    hid_ref, mem_out_ref, norm_out_ref, stab_out_ref, rows_ref,
):
    sums = in_ref[0].astype(f32)
    for z in range(1, Z):
        sums = sums + in_ref[z].astype(f32)
    for n in range(3):
        for j in range(2):
            for h in range(8):
                at = 1024 * n + 128 * h
                rows_ref[n, 8 * j + h : 8 * j + h + 1, :] = sums[j : j + 1, at : at + 128]
    extra = by_head(sums[:, 3072:3136] + sums[:, 3136:3200])
    lane = lax.broadcasted_iota(jnp.int32, extra.shape, 1)
    total = jnp.sum(jnp.where(lane == 16, extra, 0.0), axis=1, keepdims=True)
    scaling = lax.rsqrt(total / D + epsilon)
    in_gate = scaling * picked(extra, 0) + picked(jnp.broadcast_to(bi_ref[...], (16, 8)), 0)
    forget = scaling * picked(extra, 8) + picked(jnp.broadcast_to(bf_ref[...], (16, 8)), 0)
    log_forget = jnp.minimum(forget, 0.0) - jnp.log1p(jnp.exp(-jnp.abs(forget)))
    kept = picked(by_head(stab_ref[...]), 0) + log_forget
    stab_next = jnp.maximum(kept, in_gate)
    keeping = jnp.exp(kept - stab_next)
    fresh = jnp.exp(in_gate - stab_next)
    queries = (scaling * rows_ref[0]).astype(bf16).astype(f32)
    keys = (scaling * rows_ref[1]).astype(bf16).astype(f32) * 128 ** (-0.5)
    values = (scaling * rows_ref[2]).astype(bf16).astype(f32)
    norm_next = keeping * norm_ref[...] + fresh * keys
    norm_out_ref[...] = norm_next
    denominator = jnp.sum(norm_next * queries, axis=1, keepdims=True)
    denominator = jnp.maximum(jnp.abs(denominator), jnp.exp(-stab_next))
    own = lax.broadcasted_iota(jnp.int32, (16, 8), 1)
    head = lax.broadcasted_iota(jnp.int32, (16, 8), 0) % 8
    spread = jnp.where(own == head, stab_next, 0.0)
    stab_out_ref[0:1, :] = jnp.sum(spread[:8], axis=0, keepdims=True)
    stab_out_ref[1:2, :] = jnp.sum(spread[8:], axis=0, keepdims=True)
    added = jnp.concatenate([fresh * values, jnp.zeros((112, 128), f32)], axis=0).T
    column = lax.broadcasted_iota(jnp.int32, (128, 128), 1)
    numerator = jnp.zeros((128, 128), f32)
    for i in range(16):
        update = added[:, i : i + 1] * keys[i : i + 1, :]
        mem_next = keeping[i : i + 1, :] * mem_ref[i] + update
        mem_out_ref[i] = mem_next
        read = jnp.sum(mem_next * queries[i : i + 1, :], axis=1, keepdims=True)
        numerator = jnp.where(column == i, read, numerator)
    hidden = (numerator.T[:16] / denominator).astype(bf16)
    for z in range(Z):
        hid_ref[2 * z] = hidden[:8]
        hid_ref[2 * z + 1] = hidden[8:]


def spread_kernel(in_ref, out_ref):
    for n in range(out_ref.shape[0]):
        out_ref[n] = in_ref[...]


def residual_kernel(
    place_ref, hid_ref, tok_ref, w0_ref, w1_ref, w2_ref, w3_ref, other_ref, spread_ref, parts_ref
):
    first = place_ref[0] == 0
    lower, upper = hid_ref[:, :1024], hid_ref[:, 1024:]
    own = jnp.where(first, lower, upper)
    other = jnp.where(first, upper, lower)
    for step, ref in enumerate((w0_ref, w1_ref, w2_ref, w3_ref)):
        part = contracted(own, ref[...], 1, 1).astype(bf16).astype(f32)
        part = part + contracted(other, other_ref[step], 1, 1).astype(bf16).astype(f32)
        parts_ref[(place_ref[2] + Y - step) % Y] = part
    branch = jnp.concatenate([parts_ref[y] for y in range(Y)], axis=1)
    at = lax.broadcasted_iota(jnp.int32, (Z, 32), 0)
    row = lax.broadcasted_iota(jnp.int32, (Z, 32), 1)
    chosen = jnp.where(row == 2 * at + place_ref[0], 1.0, 0.0).astype(bf16)
    tok = jnp.dot(chosen, tok_ref[...], preferred_element_type=f32)
    residual = (tok + branch).astype(bf16)
    for z in range(Z):
        spread_ref[z] = residual


def mlp_kernel(
    place_ref, own_ref, other_ref, gain_ref, wg_ref, wu_ref, wd_ref,
    keep_ref, send_ref, res_ref, x_ref, block_ref,
):
    first = place_ref[0] == 0
    squares = [jnp.zeros((Z, 256), f32) for _ in range(2 * Y)]
    for z in range(Z):
        gain = gain_ref[z : z + 1, :]
        for y in range(Y):
            own = own_ref[y, Z * z : Z * (z + 1), :].astype(f32)
            other = other_ref[y, Z * z : Z * (z + 1), :].astype(f32)
            for n, x in enumerate((jnp.where(first, own, other), jnp.where(first, other, own))):
                at = Y * n + y
                squares[at] = squares[at] + x * x
                x_ref[Z * at : Z * (at + 1), 256 * z : 256 * (z + 1)] = (x * gain).astype(bf16)
    total = jnp.sum(jnp.concatenate(squares, axis=0), axis=1, keepdims=True)
    scaling = lax.rsqrt(total / D + epsilon)
    scaling = jnp.broadcast_to(scaling, (ROWS, ROWS)).T[0:1]

    here = pl.multiple_of(Z * place_ref[3], Z)
    for y in range(Y):
        own = own_ref[y, pl.ds(here, Z), :]
        other = other_ref[y, pl.ds(here, Z), :]
        block_ref[Z * y : Z * (y + 1), :] = jnp.where(first, own, other)
        block_ref[64 + Z * y : 64 + Z * (y + 1), :] = jnp.where(first, other, own)
    at = lax.broadcasted_iota(jnp.int32, (HALF, 256), 0)
    lane = lax.broadcasted_iota(jnp.int32, (HALF, 256), 1)
    chosen = jnp.where(lane == at + place_ref[1], 1.0, 0.0).astype(bf16)
    res_ref[...] = contracted(chosen, block_ref[...], 1, 1).astype(bf16)

    x = x_ref[...]
    gate = scaling * contracted(wg_ref[...], x, 1, 1)
    up = scaling * contracted(wu_ref[...], x, 1, 1)
    activated = (gate * jax.nn.sigmoid(gate) * up).astype(bf16)
    for m in range(2 * Z):
        part = contracted(wd_ref[:, 128 * m : 128 * (m + 1)], activated, 0, 0)
        z = m // 2
        for pair in range(2):
            y = 2 * (m % 2) + pair
            lower = part[64 * pair : 64 * pair + HALF]
            upper = part[64 * pair + HALF : 64 * pair + 64]
            keep_ref[y, HALF * z : HALF * (z + 1), :] = jnp.where(first, lower, upper)
            send_ref[y, HALF * z : HALF * (z + 1), :] = jnp.where(first, upper, lower).astype(bf16)


def finish_kernel(in_ref, res_ref, out_ref):
    total = res_ref[...].astype(f32)
    acc = in_ref[0].astype(f32)
    for z in range(1, Z):
        acc = acc + in_ref[z].astype(f32)
    mixed = (total + acc).astype(bf16)
    out_ref[...] = jnp.dot(mixed, row_selection(True, final_row), preferred_element_type=f32).astype(bf16)


def called(kernel, out_shape, flops=0, grant=16, **kw):
    return pl.pallas_call(
        kernel,
        out_shape=out_shape,
        cost_estimate=pl.CostEstimate(flops=flops, bytes_accessed=10**6, transcendentals=0),
        compiler_params=pltpu.CompilerParams(vmem_limit_bytes=grant * 2**20),
        **kw,
    )


IN_VMEM = pl.BlockSpec(memory_space=pltpu.VMEM)
IN_SMEM = pl.BlockSpec(memory_space=pltpu.SMEM)
IN_HBM = pl.BlockSpec(memory_space=pltpu.HBM)


def layer(
    tokens,
    gain_mix,
    w_query,
    w_key,
    w_value,
    w_igate,
    w_fgate,
    bias_igate,
    bias_fgate,
    memory,
    normalizer,
    stabilizer,
    w_output,
    gain_mlp,
    w_gate,
    w_up,
    w_down,
):
    core = lax.axis_index("tp")
    at_z, at_y = lax.axis_index("kv_0"), lax.axis_index("kv_1")
    place = jnp.stack([core, 64 * at_y + HALF * core, at_y, at_z]).astype(jnp.int32)
    shape = jax.ShapeDtypeStruct
    partials = called(
        project_kernel,
        shape((Y, 32, 3328), bf16),
        flops=2 * 64 * 128 * 3200,
        grant=60,
        in_specs=[IN_VMEM] * 4 + [IN_HBM] * 3,
        scratch_shapes=[pltpu.VMEM((3, 64, 1024), bf16), pltpu.SemaphoreType.DMA((3,))],
    )(tokens.T, gain_mix.reshape(1, 64), w_igate.T, w_fgate.T, w_query, w_key, w_value)
    w_own = w_output.T
    partials = exchanged(partials, "kv_1")
    partials, tok = called(
        sum_y_kernel, (shape((Z, 2, 3200), bf16), shape((32, 256), bf16)), flops=10**6
    )(partials)
    partials = exchanged(partials, "kv_0")
    w_all = [w_own]
    for step in range(1, Y):
        w_all.append(lax.ppermute(w_own, "kv_1", [(i, (i + step) % Y) for i in range(Y)]))
    w_other = swapped(jnp.stack(w_all))
    hidden, memory_next, norm_next, stab_next = called(
        cell_kernel,
        (
            shape((2 * Z, 8, 128), bf16),
            shape((16, 128, 128), f32),
            shape((16, 128), f32),
            shape((2, 8), f32),
        ),
        flops=10**7,
        scratch_shapes=[pltpu.VMEM((3, 16, 128), f32)],
    )(
        partials,
        bias_igate.reshape(1, 8),
        bias_fgate.reshape(1, 8),
        memory.reshape(16, 128, 128),
        normalizer.reshape(16, 128),
        stabilizer,
    )
    hidden = exchanged(hidden, ("kv_0", "tp"))
    spread = called(
        residual_kernel,
        shape((Z, Z, 256), bf16),
        flops=10**7,
        in_specs=[IN_SMEM] + [IN_VMEM] * 7,
        scratch_shapes=[pltpu.VMEM((Y, Z, 64), f32)],
    )(place, hidden.reshape(Z, 2048), tok, *w_all, w_other)
    spread = exchanged(spread, "kv_0").reshape(256, 256)
    spread = called(spread_kernel, shape((Y, 256, 256), bf16), flops=10**6)(spread)
    spread = exchanged(spread, "kv_1")
    other = swapped(spread)
    keep, send, residual = called(
        mlp_kernel,
        (
            shape((Y, BLOCK, ROWS), f32),
            shape((Y, BLOCK, ROWS), bf16),
            shape((HALF, ROWS), bf16),
        ),
        flops=6 * 128 * 88 * 4096,
        in_specs=[IN_SMEM] + [IN_VMEM] * 6,
        scratch_shapes=[pltpu.VMEM((ROWS, D), bf16), pltpu.VMEM((ROWS, 256), bf16)],
    )(place, spread, other, gain_mlp.reshape(Z, 256), w_gate.T, w_up.T, w_down)
    terms = (keep + swapped(send).astype(f32)).astype(bf16)
    terms = exchanged(terms, "kv_1").astype(f32).sum(axis=0).astype(bf16)
    terms = exchanged(terms.reshape(Z, HALF, ROWS), "kv_0")
    mixed = called(finish_kernel, shape((HALF, ROWS), bf16), flops=10**6)(terms, residual)
    return (
        mixed.T,
        memory_next.reshape(2, 8, 128, 128),
        norm_next.reshape(2, 8, 128),
        stab_next,
    )


def solution(mesh):
    torus = Mesh(
        mesh.devices.reshape(mesh.shape["dp"], Z, Y, mesh.shape["tp"]),
        ("dp", "kv_0", "kv_1", "tp"),
    )
    in_specs = (
        P("dp", KV),
        P(KV),
        P(KV, "tp"),
        P(KV, "tp"),
        P(KV, "tp"),
        P(KV, "tp"),
        P(KV, "tp"),
        P("tp"),
        P("tp"),
        P(DP_KV, "tp", None, None),
        P(DP_KV, "tp", None),
        P(DP_KV, "tp"),
        P("tp", KV),
        P(),
        P(None, KV_TP),
        P(None, KV_TP),
        P(KV_TP, None),
    )
    out_specs = (P("dp", KV_TP), P(DP_KV, "tp", None, None), P(DP_KV, "tp", None), P(DP_KV, "tp"))
    return jax.shard_map(layer, mesh=torus, in_specs=in_specs, out_specs=out_specs, check_vma=False)
```

```python
import jax
import jax.numpy as jnp
from jax import lax
from jax.experimental import pallas as pl
from jax.experimental.pallas import tpu as pltpu
from jax.sharding import Mesh
from jax.sharding import PartitionSpec as P


D = 4096
KV = ("kv_0", "kv_1")
DP_KV = ("dp", "kv_0", "kv_1")
KV_TP = ("kv_0", "kv_1", "tp")
Z, Y = 16, 4
ROWS = 128
HALF = 32
BLOCK = Z * HALF
epsilon = 1e-06
f32 = jnp.float32
bf16 = jnp.bfloat16


def exchanged(x, axis):
    return lax.all_to_all(x, axis, split_axis=0, concat_axis=0, tiled=True)


def mirrored(x):
    groups = [[0, 2, 4, 6], [7, 5, 3, 1]]
    return lax.all_to_all(
        x, ("kv_1", "tp"), split_axis=0, concat_axis=0, tiled=True, axis_index_groups=groups
    )


def swapped(x):
    return lax.ppermute(x, "tp", [(0, 1), (1, 0)])


def contracted(a, b, dim_a, dim_b):
    return lax.dot_general(a, b, (((dim_a,), (dim_b,)), ((), ())), preferred_element_type=f32)


def natural_row(i):
    return 8 * ((i // 2) % Z) + 2 * (i // 32) + i % 2


def final_row(i):
    return 8 * (i % Z) + 2 * ((i // Z) % Y) + i // 64


def row_selection(transposed, natural_row=natural_row):
    a = lax.broadcasted_iota(jnp.int32, (ROWS, ROWS), 0)
    b = lax.broadcasted_iota(jnp.int32, (ROWS, ROWS), 1)
    if transposed:
        hit = natural_row(a) == b
    else:
        hit = a == natural_row(b)
    return jnp.where(hit, 1.0, 0.0).astype(bf16)


def high_low(x):
    lane = lax.broadcasted_iota(jnp.int32, x.shape, 1)
    high = x.astype(bf16)
    low = (x - high.astype(f32)).astype(bf16)
    return jnp.where(lane < 64, high.astype(f32), low.astype(f32)).astype(bf16)


def column_of(row, count, offset=0):
    lane = lax.broadcasted_iota(jnp.int32, (count, row.shape[1]), 1)
    at = lax.broadcasted_iota(jnp.int32, (count, row.shape[1]), 0)
    return jnp.sum(jnp.where(lane == at + offset, row, 0.0), axis=1, keepdims=True)


def project_kernel(
    tok_ref, gain_ref, wi_ref, wf_ref, wq_ref, wk_ref, wv_ref, out_ref
):
    tok = jnp.dot(tok_ref[...], row_selection(False), preferred_element_type=f32)
    rows = contracted(row_selection(True), tok_ref[...], 1, 1).astype(bf16)
    out_ref[:, :, 3200:] = jnp.concatenate([rows, rows], axis=1).reshape(Y, 32, 128)
    scaled = (tok * column_of(gain_ref[...], 64)).astype(bf16)
    gates = jnp.concatenate([wi_ref[...].astype(f32), wf_ref[...].astype(f32)], axis=0)
    rest = jnp.zeros((48, 64), f32)
    gates = jnp.concatenate([gates, rest, gates, rest], axis=0).astype(bf16)
    extra = contracted(scaled, gates, 0, 1)
    squares = tok * tok
    high = squares.astype(bf16)
    low = (squares - high.astype(f32)).astype(bf16)
    lane = lax.broadcasted_iota(jnp.int32, (64, 128), 1)
    ones = jnp.where(lane % 64 == 16, 1.0, 0.0).astype(bf16)
    extra = extra + contracted(high, ones, 0, 0) + contracted(low, ones, 0, 0)
    out_ref[:, :, 3072:3200] = high_low(extra).reshape(Y, 32, 128)
    for n, ref in enumerate((wq_ref, wk_ref, wv_ref)):
        part = contracted(scaled, ref[...], 0, 0).astype(bf16)
        out_ref[:, :, 1024 * n : 1024 * (n + 1)] = part.reshape(Y, 32, 1024)


def sum_y_kernel(in_ref, out_ref, tok_ref):
    for y in range(Y):
        tok_ref[:, 64 * y : 64 * (y + 1)] = in_ref[y, :, 3200:3264]
    for n in range(3):
        cut = slice(1024 * n, 1024 * (n + 1))
        total = in_ref[0, :, cut].astype(f32)
        for y in range(1, Y):
            total = total + in_ref[y, :, cut].astype(f32)
        out_ref[:, :, cut] = total.astype(bf16).reshape(Z, 2, 1024)
    total = in_ref[0, :, 3072:3200].astype(f32)
    for y in range(1, Y):
        total = total + in_ref[y, :, 3072:3200].astype(f32)
    total = total + jnp.concatenate([total[:, 64:], total[:, :64]], axis=1)
    out_ref[:, :, 3072:] = high_low(total).reshape(Z, 2, 128)


def by_head(x):
    count = x.shape[1]
    return jnp.concatenate(
        [jnp.broadcast_to(x[0:1], (8, count)), jnp.broadcast_to(x[1:2], (8, count))], axis=0
    )


def picked(x, offset):
    lane = lax.broadcasted_iota(jnp.int32, x.shape, 1)
    head = lax.broadcasted_iota(jnp.int32, x.shape, 0) % 8
    return jnp.sum(jnp.where(lane == head + offset, x, 0.0), axis=1, keepdims=True)


def cell_kernel(
    in_ref, small_ref, mem_ref, norm_ref,
    hid_ref, mem_out_ref, norm_out_ref, stab_out_ref, rows_ref,
):
    sums = in_ref[0].astype(f32)
    for z in range(1, Z):
        sums = sums + in_ref[z].astype(f32)
    for n in range(3):
        for j in range(2):
            for h in range(8):
                at = 1024 * n + 128 * h
                rows_ref[n, 8 * j + h : 8 * j + h + 1, :] = sums[j : j + 1, at : at + 128]
    extra = by_head(sums[:, 3072:3136] + sums[:, 3136:3200])
    lane = lax.broadcasted_iota(jnp.int32, extra.shape, 1)
    total = jnp.sum(jnp.where(lane == 16, extra, 0.0), axis=1, keepdims=True)
    scaling = lax.rsqrt(total / D + epsilon)
    in_gate = scaling * picked(extra, 0) + picked(jnp.broadcast_to(small_ref[2:3, :], (16, 8)), 0)
    forget = scaling * picked(extra, 8) + picked(jnp.broadcast_to(small_ref[3:4, :], (16, 8)), 0)
    log_forget = jnp.minimum(forget, 0.0) - jnp.log1p(jnp.exp(-jnp.abs(forget)))
    kept = picked(by_head(small_ref[0:2, :]), 0) + log_forget
    stab_next = jnp.maximum(kept, in_gate)
    keeping = jnp.exp(kept - stab_next)
    fresh = jnp.exp(in_gate - stab_next)
    queries = (scaling * rows_ref[0]).astype(bf16).astype(f32)
    keys = (scaling * rows_ref[1]).astype(bf16).astype(f32) * 128 ** (-0.5)
    values = (scaling * rows_ref[2]).astype(bf16).astype(f32)
    norm_next = keeping * norm_ref[...] + fresh * keys
    norm_out_ref[...] = norm_next
    denominator = jnp.sum(norm_next * queries, axis=1, keepdims=True)
    denominator = jnp.maximum(jnp.abs(denominator), jnp.exp(-stab_next))
    own = lax.broadcasted_iota(jnp.int32, (16, 8), 1)
    head = lax.broadcasted_iota(jnp.int32, (16, 8), 0) % 8
    spread = jnp.where(own == head, stab_next, 0.0)
    stab_out_ref[0:1, :] = jnp.sum(spread[:8], axis=0, keepdims=True)
    stab_out_ref[1:2, :] = jnp.sum(spread[8:], axis=0, keepdims=True)
    added = jnp.concatenate([fresh * values, jnp.zeros((112, 128), f32)], axis=0).T
    column = lax.broadcasted_iota(jnp.int32, (128, 128), 1)
    numerator = jnp.zeros((128, 128), f32)
    for i in range(16):
        update = added[:, i : i + 1] * keys[i : i + 1, :]
        mem_next = keeping[i : i + 1, :] * mem_ref[i] + update
        mem_out_ref[i] = mem_next
        read = jnp.sum(mem_next * queries[i : i + 1, :], axis=1, keepdims=True)
        numerator = jnp.where(column == i, read, numerator)
    hidden = (numerator.T[:16] / denominator).astype(bf16)
    for z in range(Z):
        hid_ref[2 * z] = hidden[:8]
        hid_ref[2 * z + 1] = hidden[8:]


def spread_kernel(in_ref, out_ref):
    for n in range(out_ref.shape[0]):
        out_ref[n] = in_ref[...]


def residual_kernel(
    place_ref, hid_ref, tok_ref, w0_ref, w1_ref, w2_ref, w3_ref, other_ref, spread_ref, parts_ref
):
    first = place_ref[0] == 0
    lower, upper = hid_ref[:, :1024], hid_ref[:, 1024:]
    own = jnp.where(first, lower, upper)
    other = jnp.where(first, upper, lower)
    for step, ref in enumerate((w0_ref, w1_ref, w2_ref, w3_ref)):
        part = contracted(own, ref[...], 1, 1).astype(bf16).astype(f32)
        part = part + contracted(other, other_ref[step], 1, 1).astype(bf16).astype(f32)
        parts_ref[(place_ref[2] + Y - step) % Y] = part
    branch = jnp.concatenate([parts_ref[y] for y in range(Y)], axis=1)
    at = lax.broadcasted_iota(jnp.int32, (Z, 32), 0)
    row = lax.broadcasted_iota(jnp.int32, (Z, 32), 1)
    chosen = jnp.where(row == 2 * at + place_ref[0], 1.0, 0.0).astype(bf16)
    tok = jnp.dot(chosen, tok_ref[...], preferred_element_type=f32)
    residual = (tok + branch).astype(bf16)
    for z in range(Z):
        spread_ref[z] = residual


def mlp_kernel(
    place_ref, own_ref, other_ref, gain_ref, wg_ref, wu_ref, wd_ref,
    keep_ref, send_ref, res_ref, x_ref, block_ref,
):
    first = place_ref[0] == 0
    mine = [jnp.where(first, y, Y - 1 - y) for y in range(Y)]
    theirs = [jnp.where(first, Y - 1 - y, y) for y in range(Y)]
    squares = [jnp.zeros((Z, 256), f32) for _ in range(2 * Y)]
    for z in range(Z):
        gain = gain_ref[z : z + 1, :]
        for y in range(Y):
            own = own_ref[mine[y], Z * z : Z * (z + 1), :].astype(f32)
            other = other_ref[theirs[y], Z * z : Z * (z + 1), :].astype(f32)
            for n, x in enumerate((jnp.where(first, own, other), jnp.where(first, other, own))):
                at = Y * n + y
                squares[at] = squares[at] + x * x
                x_ref[Z * at : Z * (at + 1), 256 * z : 256 * (z + 1)] = (x * gain).astype(bf16)
    total = jnp.sum(jnp.concatenate(squares, axis=0), axis=1, keepdims=True)
    scaling = lax.rsqrt(total / D + epsilon)
    scaling = jnp.broadcast_to(scaling, (ROWS, ROWS)).T[0:1]

    here = pl.multiple_of(Z * place_ref[3], Z)
    for y in range(Y):
        own = own_ref[mine[y], pl.ds(here, Z), :]
        other = other_ref[theirs[y], pl.ds(here, Z), :]
        block_ref[Z * y : Z * (y + 1), :] = jnp.where(first, own, other)
        block_ref[64 + Z * y : 64 + Z * (y + 1), :] = jnp.where(first, other, own)
    at = lax.broadcasted_iota(jnp.int32, (HALF, 256), 0)
    lane = lax.broadcasted_iota(jnp.int32, (HALF, 256), 1)
    chosen = jnp.where(lane == at + place_ref[1], 1.0, 0.0).astype(bf16)
    res_ref[...] = contracted(chosen, block_ref[...], 1, 1).astype(bf16)

    x = x_ref[...]
    gate = scaling * contracted(wg_ref[...], x, 1, 1)
    up = scaling * contracted(wu_ref[...], x, 1, 1)
    activated = (gate * jax.nn.sigmoid(gate) * up).astype(bf16)
    for m in range(2 * Z):
        part = contracted(wd_ref[:, 128 * m : 128 * (m + 1)], activated, 0, 0)
        z = m // 2
        for pair in range(2):
            y = 2 * (m % 2) + pair
            lower = part[64 * pair : 64 * pair + HALF]
            upper = part[64 * pair + HALF : 64 * pair + 64]
            keep_ref[mine[y], HALF * z : HALF * (z + 1), :] = jnp.where(first, lower, upper)
            send_ref[theirs[y], HALF * z : HALF * (z + 1), :] = jnp.where(first, upper, lower).astype(bf16)


def finish_kernel(in_ref, res_ref, out_ref):
    total = res_ref[...].astype(f32)
    acc = in_ref[0].astype(f32)
    for z in range(1, Z):
        acc = acc + in_ref[z].astype(f32)
    mixed = (total + acc).astype(bf16)
    out_ref[...] = jnp.dot(mixed, row_selection(True, final_row), preferred_element_type=f32).astype(bf16)


def called(kernel, out_shape, flops=0, grant=16, **kw):
    return pl.pallas_call(
        kernel,
        out_shape=out_shape,
        cost_estimate=pl.CostEstimate(flops=flops, bytes_accessed=10**6, transcendentals=0),
        compiler_params=pltpu.CompilerParams(vmem_limit_bytes=grant * 2**20),
        **kw,
    )


IN_VMEM = pl.BlockSpec(memory_space=pltpu.VMEM)
IN_SMEM = pl.BlockSpec(memory_space=pltpu.SMEM)


def layer(
    tokens,
    gain_mix,
    w_query,
    w_key,
    w_value,
    w_igate,
    w_fgate,
    bias_igate,
    bias_fgate,
    memory,
    normalizer,
    stabilizer,
    w_output,
    gain_mlp,
    w_gate,
    w_up,
    w_down,
):
    core = lax.axis_index("tp")
    at_z, at_y = lax.axis_index("kv_0"), lax.axis_index("kv_1")
    place = jnp.stack([core, 64 * at_y + HALF * core, at_y, at_z]).astype(jnp.int32)
    shape = jax.ShapeDtypeStruct
    partials = called(
        project_kernel,
        shape((Y, 32, 3328), bf16),
        flops=2 * 64 * 128 * 3200,
        grant=60,
    )(tokens.T, gain_mix.reshape(1, 64), w_igate.T, w_fgate.T, w_query, w_key, w_value)
    w_own = w_output.T
    partials = exchanged(partials, "kv_1")
    partials, tok = called(
        sum_y_kernel, (shape((Z, 2, 3200), bf16), shape((32, 256), bf16)), flops=10**6
    )(partials)
    partials = exchanged(partials, "kv_0")
    w_all = [w_own]
    for step in range(1, Y):
        w_all.append(lax.ppermute(w_own, "kv_1", [(i, (i + step) % Y) for i in range(Y)]))
    w_other = swapped(jnp.stack(w_all))
    small = jnp.concatenate(
        [stabilizer, bias_igate.reshape(1, 8), bias_fgate.reshape(1, 8)], axis=0
    )
    hidden, memory_next, norm_next, stab_next = called(
        cell_kernel,
        (
            shape((2 * Z, 8, 128), bf16),
            shape((16, 128, 128), f32),
            shape((16, 128), f32),
            shape((2, 8), f32),
        ),
        flops=10**7,
        scratch_shapes=[pltpu.VMEM((3, 16, 128), f32)],
    )(
        partials, small, memory.reshape(16, 128, 128), normalizer.reshape(16, 128)
    )
    hidden = exchanged(hidden, ("kv_0", "tp"))
    spread = called(
        residual_kernel,
        shape((Z, Z, 256), bf16),
        flops=10**7,
        in_specs=[IN_SMEM] + [IN_VMEM] * 7,
        scratch_shapes=[pltpu.VMEM((Y, Z, 64), f32)],
    )(place, hidden.reshape(Z, 2048), tok, *w_all, w_other)
    spread = exchanged(spread, "kv_0").reshape(256, 256)
    spread = called(spread_kernel, shape((Y, 256, 256), bf16), flops=10**6)(spread)
    spread = mirrored(spread)
    other = swapped(spread)
    keep, send, residual = called(
        mlp_kernel,
        (
            shape((Y, BLOCK, ROWS), f32),
            shape((Y, BLOCK, ROWS), bf16),
            shape((HALF, ROWS), bf16),
        ),
        flops=6 * 128 * 88 * 4096,
        in_specs=[IN_SMEM] + [IN_VMEM] * 6,
        scratch_shapes=[pltpu.VMEM((ROWS, D), bf16), pltpu.VMEM((ROWS, 256), bf16)],
    )(place, spread, other, gain_mlp.reshape(Z, 256), w_gate.T, w_up.T, w_down)
    terms = (keep + swapped(send).astype(f32)).astype(bf16)
    terms = mirrored(terms).astype(f32).sum(axis=0).astype(bf16)
    terms = exchanged(terms.reshape(Z, HALF, ROWS), "kv_0")
    mixed = called(finish_kernel, shape((HALF, ROWS), bf16), flops=10**6)(terms, residual)
    return (
        mixed.T,
        memory_next.reshape(2, 8, 128, 128),
        norm_next.reshape(2, 8, 128),
        stab_next,
    )


def solution(mesh):
    torus = Mesh(
        mesh.devices.reshape(mesh.shape["dp"], Z, Y, mesh.shape["tp"]),
        ("dp", "kv_0", "kv_1", "tp"),
    )
    in_specs = (
        P("dp", KV),
        P(KV),
        P(KV, "tp"),
        P(KV, "tp"),
        P(KV, "tp"),
        P(KV, "tp"),
        P(KV, "tp"),
        P("tp"),
        P("tp"),
        P(DP_KV, "tp", None, None),
        P(DP_KV, "tp", None),
        P(DP_KV, "tp"),
        P("tp", KV),
        P(),
        P(None, KV_TP),
        P(None, KV_TP),
        P(KV_TP, None),
    )
    out_specs = (P("dp", KV_TP), P(DP_KV, "tp", None, None), P(DP_KV, "tp", None), P(DP_KV, "tp"))
    return jax.shard_map(layer, mesh=torus, in_specs=in_specs, out_specs=out_specs, check_vma=False)
```

```python
import jax
import jax.numpy as jnp
from jax import lax
from jax.experimental import pallas as pl
from jax.experimental.pallas import tpu as pltpu
from jax.sharding import Mesh
from jax.sharding import PartitionSpec as P


D = 4096
KV = ("kv_0", "kv_1")
DP_KV = ("dp", "kv_0", "kv_1")
KV_TP = ("kv_0", "kv_1", "tp")
Z, Y = 16, 4
ROWS = 128
HALF = 32
BLOCK = Z * HALF
epsilon = 1e-06
f32 = jnp.float32
bf16 = jnp.bfloat16


def exchanged(x, axis):
    return lax.all_to_all(x, axis, split_axis=0, concat_axis=0, tiled=True)


def mirrored(x):
    groups = [[0, 2, 4, 6], [5, 7, 1, 3]]
    return lax.all_to_all(
        x, ("kv_1", "tp"), split_axis=0, concat_axis=0, tiled=True, axis_index_groups=groups
    )


def swapped(x):
    return lax.ppermute(x, "tp", [(0, 1), (1, 0)])


def contracted(a, b, dim_a, dim_b):
    return lax.dot_general(a, b, (((dim_a,), (dim_b,)), ((), ())), preferred_element_type=f32)


def natural_row(i):
    return 8 * ((i // 2) % Z) + 2 * (i // 32) + i % 2


def final_row(i):
    return 8 * (i % Z) + 2 * ((i // Z) % Y) + i // 64


def row_selection(transposed, natural_row=natural_row):
    a = lax.broadcasted_iota(jnp.int32, (ROWS, ROWS), 0)
    b = lax.broadcasted_iota(jnp.int32, (ROWS, ROWS), 1)
    if transposed:
        hit = natural_row(a) == b
    else:
        hit = a == natural_row(b)
    return jnp.where(hit, 1.0, 0.0).astype(bf16)


def high_low(x):
    lane = lax.broadcasted_iota(jnp.int32, x.shape, 1)
    high = x.astype(bf16)
    low = (x - high.astype(f32)).astype(bf16)
    return jnp.where(lane < 64, high.astype(f32), low.astype(f32)).astype(bf16)


def column_of(row, count, offset=0):
    lane = lax.broadcasted_iota(jnp.int32, (count, row.shape[1]), 1)
    at = lax.broadcasted_iota(jnp.int32, (count, row.shape[1]), 0)
    return jnp.sum(jnp.where(lane == at + offset, row, 0.0), axis=1, keepdims=True)


def project_kernel(
    tok_ref, gain_ref, wi_ref, wf_ref, wq_ref, wk_ref, wv_ref, out_ref
):
    tok = jnp.dot(tok_ref[...], row_selection(False), preferred_element_type=f32)
    rows = contracted(row_selection(True), tok_ref[...], 1, 1).astype(bf16)
    out_ref[:, :, 3200:] = jnp.concatenate([rows, rows], axis=1).reshape(Y, 32, 128)
    scaled = (tok * column_of(gain_ref[...], 64)).astype(bf16)
    gates = jnp.concatenate([wi_ref[...].astype(f32), wf_ref[...].astype(f32)], axis=0)
    rest = jnp.zeros((48, 64), f32)
    gates = jnp.concatenate([gates, rest, gates, rest], axis=0).astype(bf16)
    extra = contracted(scaled, gates, 0, 1)
    squares = tok * tok
    high = squares.astype(bf16)
    low = (squares - high.astype(f32)).astype(bf16)
    lane = lax.broadcasted_iota(jnp.int32, (64, 128), 1)
    ones = jnp.where(lane % 64 == 16, 1.0, 0.0).astype(bf16)
    extra = extra + contracted(high, ones, 0, 0) + contracted(low, ones, 0, 0)
    out_ref[:, :, 3072:3200] = high_low(extra).reshape(Y, 32, 128)
    for n, ref in enumerate((wq_ref, wk_ref, wv_ref)):
        part = contracted(scaled, ref[...], 0, 0).astype(bf16)
        out_ref[:, :, 1024 * n : 1024 * (n + 1)] = part.reshape(Y, 32, 1024)


def sum_y_kernel(in_ref, out_ref, tok_ref):
    for y in range(Y):
        tok_ref[:, 64 * y : 64 * (y + 1)] = in_ref[y, :, 3200:3264]
    for n in range(3):
        cut = slice(1024 * n, 1024 * (n + 1))
        total = in_ref[0, :, cut].astype(f32)
        for y in range(1, Y):
            total = total + in_ref[y, :, cut].astype(f32)
        out_ref[:, :, cut] = total.astype(bf16).reshape(Z, 2, 1024)
    total = in_ref[0, :, 3072:3200].astype(f32)
    for y in range(1, Y):
        total = total + in_ref[y, :, 3072:3200].astype(f32)
    total = total + jnp.concatenate([total[:, 64:], total[:, :64]], axis=1)
    out_ref[:, :, 3072:] = high_low(total).reshape(Z, 2, 128)


def by_head(x):
    count = x.shape[1]
    return jnp.concatenate(
        [jnp.broadcast_to(x[0:1], (8, count)), jnp.broadcast_to(x[1:2], (8, count))], axis=0
    )


def picked(x, offset):
    lane = lax.broadcasted_iota(jnp.int32, x.shape, 1)
    head = lax.broadcasted_iota(jnp.int32, x.shape, 0) % 8
    return jnp.sum(jnp.where(lane == head + offset, x, 0.0), axis=1, keepdims=True)


def cell_kernel(
    in_ref, small_ref, mem_ref, norm_ref,
    hid_ref, mem_out_ref, norm_out_ref, stab_out_ref, rows_ref,
):
    sums = in_ref[0].astype(f32)
    for z in range(1, Z):
        sums = sums + in_ref[z].astype(f32)
    for n in range(3):
        for j in range(2):
            for h in range(8):
                at = 1024 * n + 128 * h
                rows_ref[n, 8 * j + h : 8 * j + h + 1, :] = sums[j : j + 1, at : at + 128]
    extra = by_head(sums[:, 3072:3136] + sums[:, 3136:3200])
    lane = lax.broadcasted_iota(jnp.int32, extra.shape, 1)
    total = jnp.sum(jnp.where(lane == 16, extra, 0.0), axis=1, keepdims=True)
    scaling = lax.rsqrt(total / D + epsilon)
    in_gate = scaling * picked(extra, 0) + picked(jnp.broadcast_to(small_ref[2:3, :], (16, 8)), 0)
    forget = scaling * picked(extra, 8) + picked(jnp.broadcast_to(small_ref[3:4, :], (16, 8)), 0)
    log_forget = jnp.minimum(forget, 0.0) - jnp.log1p(jnp.exp(-jnp.abs(forget)))
    kept = picked(by_head(small_ref[0:2, :]), 0) + log_forget
    stab_next = jnp.maximum(kept, in_gate)
    keeping = jnp.exp(kept - stab_next)
    fresh = jnp.exp(in_gate - stab_next)
    queries = (scaling * rows_ref[0]).astype(bf16).astype(f32)
    keys = (scaling * rows_ref[1]).astype(bf16).astype(f32) * 128 ** (-0.5)
    values = (scaling * rows_ref[2]).astype(bf16).astype(f32)
    norm_next = keeping * norm_ref[...] + fresh * keys
    norm_out_ref[...] = norm_next
    denominator = jnp.sum(norm_next * queries, axis=1, keepdims=True)
    denominator = jnp.maximum(jnp.abs(denominator), jnp.exp(-stab_next))
    own = lax.broadcasted_iota(jnp.int32, (16, 8), 1)
    head = lax.broadcasted_iota(jnp.int32, (16, 8), 0) % 8
    spread = jnp.where(own == head, stab_next, 0.0)
    stab_out_ref[0:1, :] = jnp.sum(spread[:8], axis=0, keepdims=True)
    stab_out_ref[1:2, :] = jnp.sum(spread[8:], axis=0, keepdims=True)
    added = jnp.concatenate([fresh * values, jnp.zeros((112, 128), f32)], axis=0).T
    column = lax.broadcasted_iota(jnp.int32, (128, 128), 1)
    numerator = jnp.zeros((128, 128), f32)
    for i in range(16):
        update = added[:, i : i + 1] * keys[i : i + 1, :]
        mem_next = keeping[i : i + 1, :] * mem_ref[i] + update
        mem_out_ref[i] = mem_next
        read = jnp.sum(mem_next * queries[i : i + 1, :], axis=1, keepdims=True)
        numerator = jnp.where(column == i, read, numerator)
    hidden = (numerator.T[:16] / denominator).astype(bf16)
    for z in range(Z):
        hid_ref[2 * z] = hidden[:8]
        hid_ref[2 * z + 1] = hidden[8:]


def spread_kernel(in_ref, out_ref):
    for n in range(out_ref.shape[0]):
        out_ref[n] = in_ref[...]


def residual_kernel(
    place_ref, hid_ref, tok_ref, w0_ref, w1_ref, w2_ref, w3_ref, other_ref, spread_ref, parts_ref
):
    first = place_ref[0] == 0
    lower, upper = hid_ref[:, :1024], hid_ref[:, 1024:]
    own = jnp.where(first, lower, upper)
    other = jnp.where(first, upper, lower)
    for step, ref in enumerate((w0_ref, w1_ref, w2_ref, w3_ref)):
        part = contracted(own, ref[...], 1, 1).astype(bf16).astype(f32)
        part = part + contracted(other, other_ref[step], 1, 1).astype(bf16).astype(f32)
        parts_ref[(place_ref[2] + Y - step) % Y] = part
    branch = jnp.concatenate([parts_ref[y] for y in range(Y)], axis=1)
    at = lax.broadcasted_iota(jnp.int32, (Z, 32), 0)
    row = lax.broadcasted_iota(jnp.int32, (Z, 32), 1)
    chosen = jnp.where(row == 2 * at + place_ref[0], 1.0, 0.0).astype(bf16)
    tok = jnp.dot(chosen, tok_ref[...], preferred_element_type=f32)
    residual = (tok + branch).astype(bf16)
    for z in range(Z):
        spread_ref[z] = residual


def mlp_kernel(
    place_ref, own_ref, other_ref, gain_ref, wg_ref, wu_ref, wd_ref,
    keep_ref, send_ref, res_ref, x_ref, block_ref,
):
    first = place_ref[0] == 0
    mine = [jnp.where(first, y, (y + 2) % Y) for y in range(Y)]
    theirs = [jnp.where(first, (y + 2) % Y, y) for y in range(Y)]
    squares = [jnp.zeros((Z, 256), f32) for _ in range(2 * Y)]
    for z in range(Z):
        gain = gain_ref[z : z + 1, :]
        for y in range(Y):
            own = own_ref[mine[y], Z * z : Z * (z + 1), :].astype(f32)
            other = other_ref[theirs[y], Z * z : Z * (z + 1), :].astype(f32)
            for n, x in enumerate((jnp.where(first, own, other), jnp.where(first, other, own))):
                at = Y * n + y
                squares[at] = squares[at] + x * x
                x_ref[Z * at : Z * (at + 1), 256 * z : 256 * (z + 1)] = (x * gain).astype(bf16)
    total = jnp.sum(jnp.concatenate(squares, axis=0), axis=1, keepdims=True)
    scaling = lax.rsqrt(total / D + epsilon)
    scaling = jnp.broadcast_to(scaling, (ROWS, ROWS)).T[0:1]

    here = pl.multiple_of(Z * place_ref[3], Z)
    for y in range(Y):
        own = own_ref[mine[y], pl.ds(here, Z), :]
        other = other_ref[theirs[y], pl.ds(here, Z), :]
        block_ref[Z * y : Z * (y + 1), :] = jnp.where(first, own, other)
        block_ref[64 + Z * y : 64 + Z * (y + 1), :] = jnp.where(first, other, own)
    at = lax.broadcasted_iota(jnp.int32, (HALF, 256), 0)
    lane = lax.broadcasted_iota(jnp.int32, (HALF, 256), 1)
    chosen = jnp.where(lane == at + place_ref[1], 1.0, 0.0).astype(bf16)
    res_ref[...] = contracted(chosen, block_ref[...], 1, 1).astype(bf16)

    x = x_ref[...]
    gate = scaling * contracted(wg_ref[...], x, 1, 1)
    up = scaling * contracted(wu_ref[...], x, 1, 1)
    activated = (gate * jax.nn.sigmoid(gate) * up).astype(bf16)
    for m in range(2 * Z):
        part = contracted(wd_ref[:, 128 * m : 128 * (m + 1)], activated, 0, 0)
        z = m // 2
        for pair in range(2):
            y = 2 * (m % 2) + pair
            lower = part[64 * pair : 64 * pair + HALF]
            upper = part[64 * pair + HALF : 64 * pair + 64]
            keep_ref[mine[y], HALF * z : HALF * (z + 1), :] = jnp.where(first, lower, upper)
            send_ref[theirs[y], HALF * z : HALF * (z + 1), :] = jnp.where(first, upper, lower).astype(bf16)


def finish_kernel(in_ref, res_ref, out_ref):
    total = res_ref[...].astype(f32)
    acc = in_ref[0].astype(f32)
    for z in range(1, Z):
        acc = acc + in_ref[z].astype(f32)
    mixed = (total + acc).astype(bf16)
    out_ref[...] = jnp.dot(mixed, row_selection(True, final_row), preferred_element_type=f32).astype(bf16)


def called(kernel, out_shape, flops=0, grant=16, **kw):
    return pl.pallas_call(
        kernel,
        out_shape=out_shape,
        cost_estimate=pl.CostEstimate(flops=flops, bytes_accessed=10**6, transcendentals=0),
        compiler_params=pltpu.CompilerParams(vmem_limit_bytes=grant * 2**20),
        **kw,
    )


IN_VMEM = pl.BlockSpec(memory_space=pltpu.VMEM)
IN_SMEM = pl.BlockSpec(memory_space=pltpu.SMEM)


def layer(
    tokens,
    gain_mix,
    w_query,
    w_key,
    w_value,
    w_igate,
    w_fgate,
    bias_igate,
    bias_fgate,
    memory,
    normalizer,
    stabilizer,
    w_output,
    gain_mlp,
    w_gate,
    w_up,
    w_down,
):
    core = lax.axis_index("tp")
    at_z, at_y = lax.axis_index("kv_0"), lax.axis_index("kv_1")
    place = jnp.stack([core, 64 * at_y + HALF * core, at_y, at_z]).astype(jnp.int32)
    shape = jax.ShapeDtypeStruct
    partials = called(
        project_kernel,
        shape((Y, 32, 3328), bf16),
        flops=2 * 64 * 128 * 3200,
        grant=60,
    )(tokens.T, gain_mix.reshape(1, 64), w_igate.T, w_fgate.T, w_query, w_key, w_value)
    w_own = w_output.T
    partials = exchanged(partials, "kv_1")
    partials, tok = called(
        sum_y_kernel, (shape((Z, 2, 3200), bf16), shape((32, 256), bf16)), flops=10**6
    )(partials)
    partials = exchanged(partials, "kv_0")
    w_all = [w_own]
    for step in range(1, Y):
        w_all.append(lax.ppermute(w_own, "kv_1", [(i, (i + step) % Y) for i in range(Y)]))
    w_other = swapped(jnp.stack(w_all))
    small = jnp.concatenate(
        [stabilizer, bias_igate.reshape(1, 8), bias_fgate.reshape(1, 8)], axis=0
    )
    hidden, memory_next, norm_next, stab_next = called(
        cell_kernel,
        (
            shape((2 * Z, 8, 128), bf16),
            shape((16, 128, 128), f32),
            shape((16, 128), f32),
            shape((2, 8), f32),
        ),
        flops=10**7,
        scratch_shapes=[pltpu.VMEM((3, 16, 128), f32)],
    )(
        partials, small, memory.reshape(16, 128, 128), normalizer.reshape(16, 128)
    )
    hidden = exchanged(hidden, ("kv_0", "tp"))
    spread = called(
        residual_kernel,
        shape((Z, Z, 256), bf16),
        flops=10**7,
        in_specs=[IN_SMEM] + [IN_VMEM] * 7,
        scratch_shapes=[pltpu.VMEM((Y, Z, 64), f32)],
    )(place, hidden.reshape(Z, 2048), tok, *w_all, w_other)
    spread = exchanged(spread, "kv_0").reshape(256, 256)
    spread = called(spread_kernel, shape((Y, 256, 256), bf16), flops=10**6)(spread)
    spread = mirrored(spread)
    other = swapped(spread)
    keep, send, residual = called(
        mlp_kernel,
        (
            shape((Y, BLOCK, ROWS), f32),
            shape((Y, BLOCK, ROWS), bf16),
            shape((HALF, ROWS), bf16),
        ),
        flops=6 * 128 * 88 * 4096,
        in_specs=[IN_SMEM] + [IN_VMEM] * 6,
        scratch_shapes=[pltpu.VMEM((ROWS, D), bf16), pltpu.VMEM((ROWS, 256), bf16)],
    )(place, spread, other, gain_mlp.reshape(Z, 256), w_gate.T, w_up.T, w_down)
    terms = (keep + swapped(send).astype(f32)).astype(bf16)
    terms = mirrored(terms).astype(f32).sum(axis=0).astype(bf16)
    terms = exchanged(terms.reshape(Z, HALF, ROWS), "kv_0")
    mixed = called(finish_kernel, shape((HALF, ROWS), bf16), flops=10**6)(terms, residual)
    return (
        mixed.T,
        memory_next.reshape(2, 8, 128, 128),
        norm_next.reshape(2, 8, 128),
        stab_next,
    )


def solution(mesh):
    torus = Mesh(
        mesh.devices.reshape(mesh.shape["dp"], Z, Y, mesh.shape["tp"]),
        ("dp", "kv_0", "kv_1", "tp"),
    )
    in_specs = (
        P("dp", KV),
        P(KV),
        P(KV, "tp"),
        P(KV, "tp"),
        P(KV, "tp"),
        P(KV, "tp"),
        P(KV, "tp"),
        P("tp"),
        P("tp"),
        P(DP_KV, "tp", None, None),
        P(DP_KV, "tp", None),
        P(DP_KV, "tp"),
        P("tp", KV),
        P(),
        P(None, KV_TP),
        P(None, KV_TP),
        P(KV_TP, None),
    )
    out_specs = (P("dp", KV_TP), P(DP_KV, "tp", None, None), P(DP_KV, "tp", None), P(DP_KV, "tp"))
    return jax.shard_map(layer, mesh=torus, in_specs=in_specs, out_specs=out_specs, check_vma=False)
```

```python
import jax
import jax.numpy as jnp
from jax import lax
from jax.experimental import pallas as pl
from jax.experimental.pallas import tpu as pltpu
from jax.sharding import Mesh
from jax.sharding import PartitionSpec as P


D = 4096
KV = ("kv_0", "kv_1")
DP_KV = ("dp", "kv_0", "kv_1")
KV_TP = ("kv_0", "kv_1", "tp")
Z, Y = 16, 4
ROWS = 128
HALF = 32
BLOCK = Z * HALF
epsilon = 1e-06
f32 = jnp.float32
bf16 = jnp.bfloat16


def exchanged(x, axis):
    return lax.all_to_all(x, axis, split_axis=0, concat_axis=0, tiled=True)


def mirrored(x):
    groups = [[0, 2, 4, 6], [5, 7, 1, 3]]
    return lax.all_to_all(
        x, ("kv_1", "tp"), split_axis=0, concat_axis=0, tiled=True, axis_index_groups=groups
    )


def swapped(x):
    return lax.ppermute(x, "tp", [(0, 1), (1, 0)])


def contracted(a, b, dim_a, dim_b):
    return lax.dot_general(a, b, (((dim_a,), (dim_b,)), ((), ())), preferred_element_type=f32)


def natural_row(i):
    return 8 * ((i // 2) % Z) + 2 * (i // 32) + i % 2


def final_row(i):
    return 8 * (i % Z) + 2 * ((i // Z) % Y) + i // 64


def row_selection(transposed, natural_row=natural_row):
    a = lax.broadcasted_iota(jnp.int32, (ROWS, ROWS), 0)
    b = lax.broadcasted_iota(jnp.int32, (ROWS, ROWS), 1)
    if transposed:
        hit = natural_row(a) == b
    else:
        hit = a == natural_row(b)
    return jnp.where(hit, 1.0, 0.0).astype(bf16)


def high_low(x):
    lane = lax.broadcasted_iota(jnp.int32, x.shape, 1)
    high = x.astype(bf16)
    low = (x - high.astype(f32)).astype(bf16)
    return jnp.where(lane < 64, high.astype(f32), low.astype(f32)).astype(bf16)


def column_of(row, count, offset=0):
    lane = lax.broadcasted_iota(jnp.int32, (count, row.shape[1]), 1)
    at = lax.broadcasted_iota(jnp.int32, (count, row.shape[1]), 0)
    return jnp.sum(jnp.where(lane == at + offset, row, 0.0), axis=1, keepdims=True)


def project_kernel(
    tok_ref, gain_ref, wi_ref, wf_ref, wq_ref, wk_ref, wv_ref, out_ref
):
    tok = jnp.dot(tok_ref[...], row_selection(False), preferred_element_type=f32)
    rows = contracted(row_selection(True), tok_ref[...], 1, 1).astype(bf16)
    out_ref[:, :, 3200:] = jnp.concatenate([rows, rows], axis=1).reshape(Y, 32, 128)
    scaled = (tok * column_of(gain_ref[...], 64)).astype(bf16)
    gates = jnp.concatenate([wi_ref[...].astype(f32), wf_ref[...].astype(f32)], axis=0)
    rest = jnp.zeros((48, 64), f32)
    gates = jnp.concatenate([gates, rest, gates, rest], axis=0).astype(bf16)
    extra = contracted(scaled, gates, 0, 1)
    squares = tok * tok
    high = squares.astype(bf16)
    low = (squares - high.astype(f32)).astype(bf16)
    lane = lax.broadcasted_iota(jnp.int32, (64, 128), 1)
    ones = jnp.where(lane % 64 == 16, 1.0, 0.0).astype(bf16)
    extra = extra + contracted(high, ones, 0, 0) + contracted(low, ones, 0, 0)
    out_ref[:, :, 3072:3200] = high_low(extra).reshape(Y, 32, 128)
    for n, ref in enumerate((wq_ref, wk_ref, wv_ref)):
        part = contracted(scaled, ref[...], 0, 0).astype(bf16)
        out_ref[:, :, 1024 * n : 1024 * (n + 1)] = part.reshape(Y, 32, 1024)


def sum_y_kernel(in_ref, out_ref, tok_ref):
    for y in range(Y):
        tok_ref[:, 64 * y : 64 * (y + 1)] = in_ref[y, :, 3200:3264]
    for n in range(3):
        cut = slice(1024 * n, 1024 * (n + 1))
        total = in_ref[0, :, cut].astype(f32)
        for y in range(1, Y):
            total = total + in_ref[y, :, cut].astype(f32)
        out_ref[:, :, cut] = total.astype(bf16).reshape(Z, 2, 1024)
    total = in_ref[0, :, 3072:3200].astype(f32)
    for y in range(1, Y):
        total = total + in_ref[y, :, 3072:3200].astype(f32)
    total = total + jnp.concatenate([total[:, 64:], total[:, :64]], axis=1)
    out_ref[:, :, 3072:] = high_low(total).reshape(Z, 2, 128)


def by_head(x):
    count = x.shape[1]
    return jnp.concatenate(
        [jnp.broadcast_to(x[0:1], (8, count)), jnp.broadcast_to(x[1:2], (8, count))], axis=0
    )


def picked(x, offset):
    lane = lax.broadcasted_iota(jnp.int32, x.shape, 1)
    head = lax.broadcasted_iota(jnp.int32, x.shape, 0) % 8
    return jnp.sum(jnp.where(lane == head + offset, x, 0.0), axis=1, keepdims=True)


def cell_kernel(
    in_ref, small_ref, mem_ref, norm_ref,
    hid_ref, mem_out_ref, norm_out_ref, stab_out_ref, rows_ref,
):
    sums = in_ref[0].astype(f32)
    for z in range(1, Z):
        sums = sums + in_ref[z].astype(f32)
    for n in range(3):
        for j in range(2):
            for h in range(8):
                at = 1024 * n + 128 * h
                rows_ref[n, 8 * j + h : 8 * j + h + 1, :] = sums[j : j + 1, at : at + 128]
    extra = by_head(sums[:, 3072:3136] + sums[:, 3136:3200])
    lane = lax.broadcasted_iota(jnp.int32, extra.shape, 1)
    total = jnp.sum(jnp.where(lane == 16, extra, 0.0), axis=1, keepdims=True)
    scaling = lax.rsqrt(total / D + epsilon)
    in_gate = scaling * picked(extra, 0) + picked(jnp.broadcast_to(small_ref[2:3, :], (16, 8)), 0)
    forget = scaling * picked(extra, 8) + picked(jnp.broadcast_to(small_ref[3:4, :], (16, 8)), 0)
    log_forget = jnp.minimum(forget, 0.0) - jnp.log1p(jnp.exp(-jnp.abs(forget)))
    kept = picked(by_head(small_ref[0:2, :]), 0) + log_forget
    stab_next = jnp.maximum(kept, in_gate)
    keeping = jnp.exp(kept - stab_next)
    fresh = jnp.exp(in_gate - stab_next)
    queries = (scaling * rows_ref[0]).astype(bf16).astype(f32)
    keys = (scaling * rows_ref[1]).astype(bf16).astype(f32) * 128 ** (-0.5)
    values = (scaling * rows_ref[2]).astype(bf16).astype(f32)
    norm_next = keeping * norm_ref[...] + fresh * keys
    norm_out_ref[...] = norm_next
    denominator = jnp.sum(norm_next * queries, axis=1, keepdims=True)
    denominator = jnp.maximum(jnp.abs(denominator), jnp.exp(-stab_next))
    own = lax.broadcasted_iota(jnp.int32, (16, 8), 1)
    head = lax.broadcasted_iota(jnp.int32, (16, 8), 0) % 8
    spread = jnp.where(own == head, stab_next, 0.0)
    stab_out_ref[0:1, :] = jnp.sum(spread[:8], axis=0, keepdims=True)
    stab_out_ref[1:2, :] = jnp.sum(spread[8:], axis=0, keepdims=True)
    added = jnp.concatenate([fresh * values, jnp.zeros((112, 128), f32)], axis=0).T
    column = lax.broadcasted_iota(jnp.int32, (128, 128), 1)
    numerator = jnp.zeros((128, 128), f32)
    for i in range(16):
        update = added[:, i : i + 1] * keys[i : i + 1, :]
        mem_next = keeping[i : i + 1, :] * mem_ref[i] + update
        mem_out_ref[i] = mem_next
        read = jnp.sum(mem_next * queries[i : i + 1, :], axis=1, keepdims=True)
        numerator = jnp.where(column == i, read, numerator)
    hidden = (numerator.T[:16] / denominator).astype(bf16)
    for z in range(Z):
        hid_ref[2 * z] = hidden[:8]
        hid_ref[2 * z + 1] = hidden[8:]


def spread_kernel(in_ref, out_ref):
    for n in range(out_ref.shape[0]):
        out_ref[n] = in_ref[...]


def residual_kernel(
    place_ref, hid_ref, tok_ref, w0_ref, w1_ref, w2_ref, w3_ref, other_ref, spread_ref, parts_ref
):
    first = place_ref[0] == 0
    lower, upper = hid_ref[:, :1024], hid_ref[:, 1024:]
    own = jnp.where(first, lower, upper)
    other = jnp.where(first, upper, lower)
    for step, ref in enumerate((w0_ref, w1_ref, w2_ref, w3_ref)):
        part = contracted(own, ref[...], 1, 1).astype(bf16).astype(f32)
        part = part + contracted(other, other_ref[step], 1, 1).astype(bf16).astype(f32)
        parts_ref[(place_ref[2] + Y - step) % Y] = part
    branch = jnp.concatenate([parts_ref[y] for y in range(Y)], axis=1)
    at = lax.broadcasted_iota(jnp.int32, (Z, 32), 0)
    row = lax.broadcasted_iota(jnp.int32, (Z, 32), 1)
    chosen = jnp.where(row == 2 * at + place_ref[0], 1.0, 0.0).astype(bf16)
    tok = jnp.dot(chosen, tok_ref[...], preferred_element_type=f32)
    residual = (tok + branch).astype(bf16)
    for z in range(Z):
        spread_ref[z] = residual


def mlp_kernel(
    place_ref, own_ref, other_ref, gain_ref, wg_ref, wu_ref, wd_ref,
    keep_ref, send_ref, res_ref, x_ref, block_ref,
):
    first = place_ref[0] == 0
    mine = [jnp.where(first, y, (y + 2) % Y) for y in range(Y)]
    theirs = [jnp.where(first, (y + 2) % Y, y) for y in range(Y)]
    squares = [jnp.zeros((Z, 256), f32) for _ in range(2 * Y)]
    for z in range(Z):
        gain = gain_ref[z : z + 1, :]
        for y in range(Y):
            own = own_ref[y, Z * z : Z * (z + 1), :].astype(f32)
            other = other_ref[y, Z * z : Z * (z + 1), :].astype(f32)
            for n, x in enumerate((jnp.where(first, own, other), jnp.where(first, other, own))):
                at = Y * n + y
                squares[at] = squares[at] + x * x
                x_ref[Z * at : Z * (at + 1), 256 * z : 256 * (z + 1)] = (x * gain).astype(bf16)
    total = jnp.sum(jnp.concatenate(squares, axis=0), axis=1, keepdims=True)
    scaling = lax.rsqrt(total / D + epsilon)
    scaling = jnp.broadcast_to(scaling, (ROWS, ROWS)).T[0:1]

    here = pl.multiple_of(Z * place_ref[3], Z)
    for y in range(Y):
        own = own_ref[y, pl.ds(here, Z), :]
        other = other_ref[y, pl.ds(here, Z), :]
        block_ref[Z * y : Z * (y + 1), :] = jnp.where(first, own, other)
        block_ref[64 + Z * y : 64 + Z * (y + 1), :] = jnp.where(first, other, own)
    at = lax.broadcasted_iota(jnp.int32, (HALF, 256), 0)
    lane = lax.broadcasted_iota(jnp.int32, (HALF, 256), 1)
    chosen = jnp.where(lane == at + place_ref[1], 1.0, 0.0).astype(bf16)
    res_ref[...] = contracted(chosen, block_ref[...], 1, 1).astype(bf16)

    x = x_ref[...]
    gate = scaling * contracted(wg_ref[...], x, 1, 1)
    up = scaling * contracted(wu_ref[...], x, 1, 1)
    activated = (gate * jax.nn.sigmoid(gate) * up).astype(bf16)
    for m in range(2 * Z):
        part = contracted(wd_ref[:, 128 * m : 128 * (m + 1)], activated, 0, 0)
        z = m // 2
        for pair in range(2):
            y = 2 * (m % 2) + pair
            lower = part[64 * pair : 64 * pair + HALF]
            upper = part[64 * pair + HALF : 64 * pair + 64]
            keep_ref[mine[y], HALF * z : HALF * (z + 1), :] = jnp.where(first, lower, upper)
            send_ref[theirs[y], HALF * z : HALF * (z + 1), :] = jnp.where(first, upper, lower).astype(bf16)


def finish_kernel(in_ref, res_ref, out_ref):
    total = res_ref[...].astype(f32)
    acc = in_ref[0].astype(f32)
    for z in range(1, Z):
        acc = acc + in_ref[z].astype(f32)
    mixed = (total + acc).astype(bf16)
    out_ref[...] = jnp.dot(mixed, row_selection(True, final_row), preferred_element_type=f32).astype(bf16)


def called(kernel, out_shape, flops=0, grant=16, **kw):
    return pl.pallas_call(
        kernel,
        out_shape=out_shape,
        cost_estimate=pl.CostEstimate(flops=flops, bytes_accessed=10**6, transcendentals=0),
        compiler_params=pltpu.CompilerParams(vmem_limit_bytes=grant * 2**20),
        **kw,
    )


IN_VMEM = pl.BlockSpec(memory_space=pltpu.VMEM)
IN_SMEM = pl.BlockSpec(memory_space=pltpu.SMEM)


def layer(
    tokens,
    gain_mix,
    w_query,
    w_key,
    w_value,
    w_igate,
    w_fgate,
    bias_igate,
    bias_fgate,
    memory,
    normalizer,
    stabilizer,
    w_output,
    gain_mlp,
    w_gate,
    w_up,
    w_down,
):
    core = lax.axis_index("tp")
    at_z, at_y = lax.axis_index("kv_0"), lax.axis_index("kv_1")
    place = jnp.stack([core, 64 * at_y + HALF * core, at_y, at_z]).astype(jnp.int32)
    shape = jax.ShapeDtypeStruct
    partials = called(
        project_kernel,
        shape((Y, 32, 3328), bf16),
        flops=2 * 64 * 128 * 3200,
        grant=60,
    )(tokens.T, gain_mix.reshape(1, 64), w_igate.T, w_fgate.T, w_query, w_key, w_value)
    w_own = w_output.T
    partials = exchanged(partials, "kv_1")
    partials, tok = called(
        sum_y_kernel, (shape((Z, 2, 3200), bf16), shape((32, 256), bf16)), flops=10**6
    )(partials)
    partials = exchanged(partials, "kv_0")
    w_all = [w_own]
    for step in range(1, Y):
        w_all.append(lax.ppermute(w_own, "kv_1", [(i, (i + step) % Y) for i in range(Y)]))
    w_other = swapped(jnp.stack(w_all))
    small = jnp.concatenate(
        [stabilizer, bias_igate.reshape(1, 8), bias_fgate.reshape(1, 8)], axis=0
    )
    hidden, memory_next, norm_next, stab_next = called(
        cell_kernel,
        (
            shape((2 * Z, 8, 128), bf16),
            shape((16, 128, 128), f32),
            shape((16, 128), f32),
            shape((2, 8), f32),
        ),
        flops=10**7,
        scratch_shapes=[pltpu.VMEM((3, 16, 128), f32)],
    )(
        partials, small, memory.reshape(16, 128, 128), normalizer.reshape(16, 128)
    )
    hidden = exchanged(hidden, ("kv_0", "tp"))
    spread = called(
        residual_kernel,
        shape((Z, Z, 256), bf16),
        flops=10**7,
        in_specs=[IN_SMEM] + [IN_VMEM] * 7,
        scratch_shapes=[pltpu.VMEM((Y, Z, 64), f32)],
    )(place, hidden.reshape(Z, 2048), tok, *w_all, w_other)
    spread = exchanged(spread, "kv_0").reshape(256, 256)
    spread = called(spread_kernel, shape((Y, 256, 256), bf16), flops=10**6)(spread)
    spread = exchanged(spread, "kv_1")
    other = swapped(spread)
    keep, send, residual = called(
        mlp_kernel,
        (
            shape((Y, BLOCK, ROWS), f32),
            shape((Y, BLOCK, ROWS), bf16),
            shape((HALF, ROWS), bf16),
        ),
        flops=6 * 128 * 88 * 4096,
        in_specs=[IN_SMEM] + [IN_VMEM] * 6,
        scratch_shapes=[pltpu.VMEM((ROWS, D), bf16), pltpu.VMEM((ROWS, 256), bf16)],
    )(place, spread, other, gain_mlp.reshape(Z, 256), w_gate.T, w_up.T, w_down)
    terms = (keep + swapped(send).astype(f32)).astype(bf16)
    terms = mirrored(terms).astype(f32).sum(axis=0).astype(bf16)
    terms = exchanged(terms.reshape(Z, HALF, ROWS), "kv_0")
    mixed = called(finish_kernel, shape((HALF, ROWS), bf16), flops=10**6)(terms, residual)
    return (
        mixed.T,
        memory_next.reshape(2, 8, 128, 128),
        norm_next.reshape(2, 8, 128),
        stab_next,
    )


def solution(mesh):
    torus = Mesh(
        mesh.devices.reshape(mesh.shape["dp"], Z, Y, mesh.shape["tp"]),
        ("dp", "kv_0", "kv_1", "tp"),
    )
    in_specs = (
        P("dp", KV),
        P(KV),
        P(KV, "tp"),
        P(KV, "tp"),
        P(KV, "tp"),
        P(KV, "tp"),
        P(KV, "tp"),
        P("tp"),
        P("tp"),
        P(DP_KV, "tp", None, None),
        P(DP_KV, "tp", None),
        P(DP_KV, "tp"),
        P("tp", KV),
        P(),
        P(None, KV_TP),
        P(None, KV_TP),
        P(KV_TP, None),
    )
    out_specs = (P("dp", KV_TP), P(DP_KV, "tp", None, None), P(DP_KV, "tp", None), P(DP_KV, "tp"))
    return jax.shard_map(layer, mesh=torus, in_specs=in_specs, out_specs=out_specs, check_vma=False)
```

```python
import jax
import jax.numpy as jnp
from jax import lax
from jax.experimental import pallas as pl
from jax.experimental.pallas import tpu as pltpu
from jax.sharding import Mesh
from jax.sharding import PartitionSpec as P


D = 4096
KV = ("kv_0", "kv_1")
DP_KV = ("dp", "kv_0", "kv_1")
KV_TP = ("kv_0", "kv_1", "tp")
Z, Y = 16, 4
ROWS = 128
HALF = 32
BLOCK = Z * HALF
epsilon = 1e-06
f32 = jnp.float32
bf16 = jnp.bfloat16


def exchanged(x, axis):
    return lax.all_to_all(x, axis, split_axis=0, concat_axis=0, tiled=True)


def mirrored(x):
    groups = [[0, 2, 4, 6], [5, 7, 1, 3]]
    return lax.all_to_all(
        x, ("kv_1", "tp"), split_axis=0, concat_axis=0, tiled=True, axis_index_groups=groups
    )


def swapped(x):
    return lax.ppermute(x, "tp", [(0, 1), (1, 0)])


def contracted(a, b, dim_a, dim_b):
    return lax.dot_general(a, b, (((dim_a,), (dim_b,)), ((), ())), preferred_element_type=f32)


def natural_row(i):
    return 8 * ((i // 2) % Z) + 2 * (i // 32) + i % 2


def final_row(i):
    return 8 * (i % Z) + 2 * ((i // Z) % Y) + i // 64


def row_selection(transposed, natural_row=natural_row):
    a = lax.broadcasted_iota(jnp.int32, (ROWS, ROWS), 0)
    b = lax.broadcasted_iota(jnp.int32, (ROWS, ROWS), 1)
    if transposed:
        hit = natural_row(a) == b
    else:
        hit = a == natural_row(b)
    return jnp.where(hit, 1.0, 0.0).astype(bf16)


def high_low(x):
    lane = lax.broadcasted_iota(jnp.int32, x.shape, 1)
    high = x.astype(bf16)
    low = (x - high.astype(f32)).astype(bf16)
    return jnp.where(lane < 64, high.astype(f32), low.astype(f32)).astype(bf16)


def column_of(row, count, offset=0):
    lane = lax.broadcasted_iota(jnp.int32, (count, row.shape[1]), 1)
    at = lax.broadcasted_iota(jnp.int32, (count, row.shape[1]), 0)
    return jnp.sum(jnp.where(lane == at + offset, row, 0.0), axis=1, keepdims=True)


def project_kernel(
    tok_ref, gain_ref, wi_ref, wf_ref, wq_ref, wk_ref, wv_ref, out_ref
):
    tok = jnp.dot(tok_ref[...], row_selection(False), preferred_element_type=f32)
    rows = contracted(row_selection(True), tok_ref[...], 1, 1).astype(bf16)
    out_ref[:, :, 3200:] = jnp.concatenate([rows, rows], axis=1).reshape(Y, 32, 128)
    scaled = (tok * column_of(gain_ref[...], 64)).astype(bf16)
    gates = jnp.concatenate([wi_ref[...].astype(f32), wf_ref[...].astype(f32)], axis=0)
    rest = jnp.zeros((48, 64), f32)
    gates = jnp.concatenate([gates, rest, gates, rest], axis=0).astype(bf16)
    extra = contracted(scaled, gates, 0, 1)
    squares = tok * tok
    high = squares.astype(bf16)
    low = (squares - high.astype(f32)).astype(bf16)
    lane = lax.broadcasted_iota(jnp.int32, (64, 128), 1)
    ones = jnp.where(lane % 64 == 16, 1.0, 0.0).astype(bf16)
    extra = extra + contracted(high, ones, 0, 0) + contracted(low, ones, 0, 0)
    out_ref[:, :, 3072:3200] = high_low(extra).reshape(Y, 32, 128)
    for n, ref in enumerate((wq_ref, wk_ref, wv_ref)):
        part = contracted(scaled, ref[...], 0, 0).astype(bf16)
        out_ref[:, :, 1024 * n : 1024 * (n + 1)] = part.reshape(Y, 32, 1024)


def sum_y_kernel(in_ref, out_ref, tok_ref):
    for y in range(Y):
        tok_ref[:, 64 * y : 64 * (y + 1)] = in_ref[y, :, 3200:3264]
    for n in range(3):
        cut = slice(1024 * n, 1024 * (n + 1))
        total = in_ref[0, :, cut].astype(f32)
        for y in range(1, Y):
            total = total + in_ref[y, :, cut].astype(f32)
        out_ref[:, :, cut] = total.astype(bf16).reshape(Z, 2, 1024)
    total = in_ref[0, :, 3072:3200].astype(f32)
    for y in range(1, Y):
        total = total + in_ref[y, :, 3072:3200].astype(f32)
    total = total + jnp.concatenate([total[:, 64:], total[:, :64]], axis=1)
    out_ref[:, :, 3072:] = high_low(total).reshape(Z, 2, 128)


def by_head(x):
    count = x.shape[1]
    return jnp.concatenate(
        [jnp.broadcast_to(x[0:1], (8, count)), jnp.broadcast_to(x[1:2], (8, count))], axis=0
    )


def picked(x, offset):
    lane = lax.broadcasted_iota(jnp.int32, x.shape, 1)
    head = lax.broadcasted_iota(jnp.int32, x.shape, 0) % 8
    return jnp.sum(jnp.where(lane == head + offset, x, 0.0), axis=1, keepdims=True)


def cell_kernel(
    in_ref, small_ref, mem_ref, norm_ref,
    hid_ref, mem_out_ref, norm_out_ref, stab_out_ref, rows_ref,
):
    sums = in_ref[0].astype(f32)
    for z in range(1, Z):
        sums = sums + in_ref[z].astype(f32)
    for n in range(3):
        for j in range(2):
            for h in range(8):
                at = 1024 * n + 128 * h
                rows_ref[n, 8 * j + h : 8 * j + h + 1, :] = sums[j : j + 1, at : at + 128]
    extra = by_head(sums[:, 3072:3136] + sums[:, 3136:3200])
    lane = lax.broadcasted_iota(jnp.int32, extra.shape, 1)
    total = jnp.sum(jnp.where(lane == 16, extra, 0.0), axis=1, keepdims=True)
    scaling = lax.rsqrt(total / D + epsilon)
    in_gate = scaling * picked(extra, 0) + picked(jnp.broadcast_to(small_ref[2:3, :], (16, 8)), 0)
    forget = scaling * picked(extra, 8) + picked(jnp.broadcast_to(small_ref[3:4, :], (16, 8)), 0)
    log_forget = jnp.minimum(forget, 0.0) - jnp.log1p(jnp.exp(-jnp.abs(forget)))
    kept = picked(by_head(small_ref[0:2, :]), 0) + log_forget
    stab_next = jnp.maximum(kept, in_gate)
    keeping = jnp.exp(kept - stab_next)
    fresh = jnp.exp(in_gate - stab_next)
    queries = (scaling * rows_ref[0]).astype(bf16).astype(f32)
    keys = (scaling * rows_ref[1]).astype(bf16).astype(f32) * 128 ** (-0.5)
    values = (scaling * rows_ref[2]).astype(bf16).astype(f32)
    norm_next = keeping * norm_ref[...] + fresh * keys
    norm_out_ref[...] = norm_next
    denominator = jnp.sum(norm_next * queries, axis=1, keepdims=True)
    denominator = jnp.maximum(jnp.abs(denominator), jnp.exp(-stab_next))
    own = lax.broadcasted_iota(jnp.int32, (16, 8), 1)
    head = lax.broadcasted_iota(jnp.int32, (16, 8), 0) % 8
    spread = jnp.where(own == head, stab_next, 0.0)
    stab_out_ref[0:1, :] = jnp.sum(spread[:8], axis=0, keepdims=True)
    stab_out_ref[1:2, :] = jnp.sum(spread[8:], axis=0, keepdims=True)
    added = jnp.concatenate([fresh * values, jnp.zeros((112, 128), f32)], axis=0).T
    column = lax.broadcasted_iota(jnp.int32, (128, 128), 1)
    numerator = jnp.zeros((128, 128), f32)
    for i in range(16):
        update = added[:, i : i + 1] * keys[i : i + 1, :]
        mem_next = keeping[i : i + 1, :] * mem_ref[i] + update
        mem_out_ref[i] = mem_next
        read = jnp.sum(mem_next * queries[i : i + 1, :], axis=1, keepdims=True)
        numerator = jnp.where(column == i, read, numerator)
    hidden = (numerator.T[:16] / denominator).astype(bf16)
    for z in range(Z):
        hid_ref[2 * z] = hidden[:8]
        hid_ref[2 * z + 1] = hidden[8:]


def spread_kernel(in_ref, out_ref):
    for n in range(out_ref.shape[0]):
        out_ref[n] = in_ref[...]


def residual_kernel(
    place_ref, hid_ref, tok_ref, w0_ref, w1_ref, w2_ref, w3_ref, other_ref, spread_ref, parts_ref
):
    first = place_ref[0] == 0
    lower, upper = hid_ref[:, :1024], hid_ref[:, 1024:]
    own = jnp.where(first, lower, upper)
    other = jnp.where(first, upper, lower)
    for step, ref in enumerate((w0_ref, w1_ref, w2_ref, w3_ref)):
        part = contracted(own, ref[...], 1, 1).astype(bf16).astype(f32)
        part = part + contracted(other, other_ref[step], 1, 1).astype(bf16).astype(f32)
        parts_ref[(place_ref[2] + Y - step) % Y] = part
    branch = jnp.concatenate([parts_ref[y] for y in range(Y)], axis=1)
    at = lax.broadcasted_iota(jnp.int32, (Z, 32), 0)
    row = lax.broadcasted_iota(jnp.int32, (Z, 32), 1)
    chosen = jnp.where(row == 2 * at + place_ref[0], 1.0, 0.0).astype(bf16)
    tok = jnp.dot(chosen, tok_ref[...], preferred_element_type=f32)
    residual = (tok + branch).astype(bf16)
    for z in range(Z):
        spread_ref[z] = residual


def mlp_kernel(
    place_ref, own_ref, other_ref, gain_ref, wg_ref, wu_ref, wd_ref,
    keep_ref, send_ref, res_ref, x_ref, block_ref,
):
    first = place_ref[0] == 0
    mine = [jnp.where(first, y, (y + 2) % Y) for y in range(Y)]
    theirs = [jnp.where(first, (y + 2) % Y, y) for y in range(Y)]
    squares = [jnp.zeros((Z, 256), f32) for _ in range(2 * Y)]
    for z in range(Z):
        gain = gain_ref[z : z + 1, :]
        for y in range(Y):
            own = own_ref[y, Z * z : Z * (z + 1), :].astype(f32)
            other = other_ref[y, Z * z : Z * (z + 1), :].astype(f32)
            for n, x in enumerate((jnp.where(first, own, other), jnp.where(first, other, own))):
                at = Y * n + y
                squares[at] = squares[at] + x * x
                x_ref[Z * at : Z * (at + 1), 256 * z : 256 * (z + 1)] = (x * gain).astype(bf16)
    total = jnp.sum(jnp.concatenate(squares, axis=0), axis=1, keepdims=True)
    scaling = lax.rsqrt(total / D + epsilon)
    scaling = jnp.broadcast_to(scaling, (ROWS, ROWS)).T[0:1]

    here = pl.multiple_of(Z * place_ref[3], Z)
    for y in range(Y):
        own = own_ref[y, pl.ds(here, Z), :]
        other = other_ref[y, pl.ds(here, Z), :]
        block_ref[Z * y : Z * (y + 1), :] = jnp.where(first, own, other)
        block_ref[64 + Z * y : 64 + Z * (y + 1), :] = jnp.where(first, other, own)
    at = lax.broadcasted_iota(jnp.int32, (HALF, 256), 0)
    lane = lax.broadcasted_iota(jnp.int32, (HALF, 256), 1)
    chosen = jnp.where(lane == at + place_ref[1], 1.0, 0.0).astype(bf16)
    res_ref[...] = contracted(chosen, block_ref[...], 1, 1).astype(bf16)

    x = x_ref[...]
    gate = scaling * contracted(wg_ref[...], x, 1, 1)
    up = scaling * contracted(wu_ref[...], x, 1, 1)
    activated = (gate * jax.nn.sigmoid(gate) * up).astype(bf16)
    for m in range(2 * Z):
        part = contracted(wd_ref[:, 128 * m : 128 * (m + 1)], activated, 0, 0)
        z = m // 2
        for pair in range(2):
            y = 2 * (m % 2) + pair
            lower = part[64 * pair : 64 * pair + HALF]
            upper = part[64 * pair + HALF : 64 * pair + 64]
            keep_ref[mine[y], HALF * z : HALF * (z + 1), :] = jnp.where(first, lower, upper).astype(bf16)
            send_ref[theirs[y], HALF * z : HALF * (z + 1), :] = jnp.where(first, upper, lower).astype(bf16)


def finish_kernel(in_ref, res_ref, out_ref):
    total = res_ref[...].astype(f32)
    acc = in_ref[0].astype(f32)
    for z in range(1, Z):
        acc = acc + in_ref[z].astype(f32)
    mixed = (total + acc).astype(bf16)
    out_ref[...] = jnp.dot(mixed, row_selection(True, final_row), preferred_element_type=f32).astype(bf16)


def called(kernel, out_shape, flops=0, grant=16, **kw):
    return pl.pallas_call(
        kernel,
        out_shape=out_shape,
        cost_estimate=pl.CostEstimate(flops=flops, bytes_accessed=10**6, transcendentals=0),
        compiler_params=pltpu.CompilerParams(vmem_limit_bytes=grant * 2**20),
        **kw,
    )


IN_VMEM = pl.BlockSpec(memory_space=pltpu.VMEM)
IN_SMEM = pl.BlockSpec(memory_space=pltpu.SMEM)


def layer(
    tokens,
    gain_mix,
    w_query,
    w_key,
    w_value,
    w_igate,
    w_fgate,
    bias_igate,
    bias_fgate,
    memory,
    normalizer,
    stabilizer,
    w_output,
    gain_mlp,
    w_gate,
    w_up,
    w_down,
):
    core = lax.axis_index("tp")
    at_z, at_y = lax.axis_index("kv_0"), lax.axis_index("kv_1")
    place = jnp.stack([core, 64 * at_y + HALF * core, at_y, at_z]).astype(jnp.int32)
    shape = jax.ShapeDtypeStruct
    partials = called(
        project_kernel,
        shape((Y, 32, 3328), bf16),
        flops=2 * 64 * 128 * 3200,
        grant=60,
    )(tokens.T, gain_mix.reshape(1, 64), w_igate.T, w_fgate.T, w_query, w_key, w_value)
    w_own = w_output.T
    partials = exchanged(partials, "kv_1")
    partials, tok = called(
        sum_y_kernel, (shape((Z, 2, 3200), bf16), shape((32, 256), bf16)), flops=10**6
    )(partials)
    partials = exchanged(partials, "kv_0")
    w_all = [w_own]
    for step in range(1, Y):
        w_all.append(lax.ppermute(w_own, "kv_1", [(i, (i + step) % Y) for i in range(Y)]))
    w_other = swapped(jnp.stack(w_all))
    small = jnp.concatenate(
        [stabilizer, bias_igate.reshape(1, 8), bias_fgate.reshape(1, 8)], axis=0
    )
    hidden, memory_next, norm_next, stab_next = called(
        cell_kernel,
        (
            shape((2 * Z, 8, 128), bf16),
            shape((16, 128, 128), f32),
            shape((16, 128), f32),
            shape((2, 8), f32),
        ),
        flops=10**7,
        scratch_shapes=[pltpu.VMEM((3, 16, 128), f32)],
    )(
        partials, small, memory.reshape(16, 128, 128), normalizer.reshape(16, 128)
    )
    hidden = exchanged(hidden, ("kv_0", "tp"))
    spread = called(
        residual_kernel,
        shape((Z, Z, 256), bf16),
        flops=10**7,
        in_specs=[IN_SMEM] + [IN_VMEM] * 7,
        scratch_shapes=[pltpu.VMEM((Y, Z, 64), f32)],
    )(place, hidden.reshape(Z, 2048), tok, *w_all, w_other)
    spread = exchanged(spread, "kv_0").reshape(256, 256)
    spread = called(spread_kernel, shape((Y, 256, 256), bf16), flops=10**6)(spread)
    spread = exchanged(spread, "kv_1")
    other = swapped(spread)
    keep, send, residual = called(
        mlp_kernel,
        (
            shape((Y, BLOCK, ROWS), bf16),
            shape((Y, BLOCK, ROWS), bf16),
            shape((HALF, ROWS), bf16),
        ),
        flops=6 * 128 * 88 * 4096,
        in_specs=[IN_SMEM] + [IN_VMEM] * 6,
        scratch_shapes=[pltpu.VMEM((ROWS, D), bf16), pltpu.VMEM((ROWS, 256), bf16)],
    )(place, spread, other, gain_mlp.reshape(Z, 256), w_gate.T, w_up.T, w_down)
    terms = (keep.astype(f32) + swapped(send).astype(f32)).astype(bf16)
    terms = mirrored(terms).astype(f32).sum(axis=0).astype(bf16)
    terms = exchanged(terms.reshape(Z, HALF, ROWS), "kv_0")
    mixed = called(finish_kernel, shape((HALF, ROWS), bf16), flops=10**6)(terms, residual)
    return (
        mixed.T,
        memory_next.reshape(2, 8, 128, 128),
        norm_next.reshape(2, 8, 128),
        stab_next,
    )


def solution(mesh):
    torus = Mesh(
        mesh.devices.reshape(mesh.shape["dp"], Z, Y, mesh.shape["tp"]),
        ("dp", "kv_0", "kv_1", "tp"),
    )
    in_specs = (
        P("dp", KV),
        P(KV),
        P(KV, "tp"),
        P(KV, "tp"),
        P(KV, "tp"),
        P(KV, "tp"),
        P(KV, "tp"),
        P("tp"),
        P("tp"),
        P(DP_KV, "tp", None, None),
        P(DP_KV, "tp", None),
        P(DP_KV, "tp"),
        P("tp", KV),
        P(),
        P(None, KV_TP),
        P(None, KV_TP),
        P(KV_TP, None),
    )
    out_specs = (P("dp", KV_TP), P(DP_KV, "tp", None, None), P(DP_KV, "tp", None), P(DP_KV, "tp"))
    return jax.shard_map(layer, mesh=torus, in_specs=in_specs, out_specs=out_specs, check_vma=False)
```
